32 devices in a mesh: row: 4 (over z), col: 8 (over y, x, core).
Axes of the slice: x: 2, y: 2, z: 4, core: 2. Of those that a mesh axis runs over, the one named last changes fastest.
Arguments:
- tokens: bfloat16 [32, 144, 2048], P('row', 'col'), may hold values from -6 to 6
- norm_gain: bfloat16 [2048], replicated, may hold values from 0.099609375 to 1.8984375
- w_in: bfloat16 [2048, 1152], replicated, may hold values from -0.125 to 0.125
- w_out: bfloat16 [1152, 2048], replicated, may hold values from -0.1875 to 0.1875
Outputs:
- mixed: bfloat16 [144, 32, 2048], P('row', 'col')
The draws below stay inside these ranges and needn't reach their ends.
All inputs are finite; a program needn't handle non-finite values.
Results may differ from the reference program's by a relative error of at most 0.013.
Values may be sent and summed in bfloat16 or wider, within the bound.
A program may use at most 64 MiB of HBM per device.

```python
import jax
import jax.numpy as jnp
from jax import lax

D = 2048
GROUP = 128
F = 1152
LEN_A = 32
LEN_B = 144
N_COL = 8


def level_of(stream_key, dims, cuts, low, high):
    level = 1.0
    for axis_at, parts in cuts:
        draws = jax.random.uniform(jax.random.fold_in(jax.random.fold_in(stream_key, 6), axis_at), (parts,), jnp.float32, low / len(cuts), high / len(cuts))
        level = level * jnp.repeat(jnp.exp(draws), dims[axis_at] // parts).reshape((-1,) + (1,) * (len(dims) - 1 - axis_at))
    return level


def gaussian(stream_key, dims, scale, bound, cuts=(), kind=jnp.bfloat16):
    array = scale * jax.random.normal(stream_key, dims, jnp.float32)
    if cuts:
        array = array * level_of(stream_key, dims, cuts, -0.22, 0.18)
    return jnp.clip(array, -bound, bound).astype(kind)


def setup_inputs(seed: int = 0) -> dict:
    arg_keys = jax.random.split(jax.random.key(seed), 5)
    tokens = gaussian(arg_keys[0], (LEN_A, LEN_B, D), 1.0, 6.0, ((0, 4), (1, 8)))
    norm_gain = jnp.clip(1.0 + 0.18 * jax.random.normal(arg_keys[1], (D,), jnp.float32), 0.099609375, 1.8984375).astype(jnp.bfloat16)
    w_in = gaussian(arg_keys[2], (D, F), D ** -0.5, 0.125)
    w_out = gaussian(arg_keys[3], (F, D), F ** -0.5, 0.1875)
    return dict(tokens=tokens, norm_gain=norm_gain, w_in=w_in, w_out=w_out)


norm_eps = 1e-06

def folded_order(length_first, devices):
    block = length_first // devices
    half_block = block // 2
    series = jnp.arange(length_first, dtype=jnp.int32)
    device = series // block
    inner = series % block
    lower = device * half_block + inner
    upper = length_first - device * half_block - (inner - half_block)
    upper = jnp.where((device == 0) & (inner == half_block), length_first // 2, upper)
    return (jnp.where(inner < half_block, lower, upper) % length_first).astype(jnp.int32)

def reference(tokens, norm_gain, w_in, w_out):
    length_first, length_second, features = tokens.shape
    positions = length_first * length_second
    floats = tokens.astype(jnp.float32).reshape(positions, features)
    normed = (floats * lax.rsqrt(lax.optimization_barrier(jnp.mean(floats * floats, axis=-1, keepdims=True)) + norm_eps) * norm_gain.astype(jnp.float32)).astype(jnp.bfloat16)
    mapped = jnp.dot(normed, w_in, preferred_element_type=jnp.float32).astype(jnp.bfloat16)
    channels = mapped.shape[1]
    grouped = mapped.astype(jnp.float32).reshape(positions, channels // GROUP, GROUP).transpose(1, 0, 2)

    def one_group(block):
        return jnp.fft.fft2(block, norm='ortho').real.astype(jnp.float32)
    spectrum = lax.map(one_group, grouped).transpose(1, 0, 2).reshape(positions, channels)
    spectrum = spectrum.astype(jnp.bfloat16)
    mixed = jnp.dot(spectrum, w_out, preferred_element_type=jnp.float32).astype(jnp.bfloat16)
    mixed = mixed.reshape(length_second, length_first, features)
    return jnp.take(mixed, folded_order(length_first, N_COL), axis=1)
```

```python
import functools
import math

import jax
import jax.numpy as jnp
import numpy as np
from jax import lax
from jax.experimental import pallas as pl
from jax.experimental.pallas import tpu as pltpu
from jax.sharding import PartitionSpec as P

GROUP = 128
LANES = 128
SUBLANES = 16
MESH = pl.DeviceIdType.MESH


norm_eps = 1e-06
highest = lax.Precision.HIGHEST


def folded_list(length_first, devices):
    block = length_first // devices
    half = block // 2
    result = np.zeros(length_first, np.int64)
    for device in range(devices):
        for inner in range(block):
            if inner < half:
                value = device * half + inner
            elif device == 0 and inner == half:
                value = length_first // 2
            else:
                value = length_first - device * half - (inner - half)
            result[device * block + inner] = value % length_first
    return result


def channel_tables(row_count):
    width = GROUP // row_count
    half = width // 2
    per_tile = LANES // width
    j = np.arange(GROUP)
    forward = np.zeros((row_count, per_tile * GROUP, LANES))
    back = np.zeros((row_count, LANES, per_tile * GROUP))
    for row in range(row_count):
        for x in range(width):
            m = row * half + x % half
            cosine = x < half
            column = np.cos(2 * np.pi * j * m / GROUP) if cosine else np.sin(2 * np.pi * j * m / GROUP)
            entries = [(m, 1.0)]
            if not cosine and m == 0:
                column = np.cos(np.pi * j)
                entries = [(GROUP // 2, 1.0)]
            elif m:
                entries = [(m, 1.0 if cosine else -1.0), (GROUP - m, 1.0)]
            for g in range(per_tile):
                forward[row, g * GROUP : (g + 1) * GROUP, g * width + x] = column
                for at, sign in entries:
                    back[row, g * width + x, g * GROUP + at] = sign
    return forward, back


def position_tables(rows_first, rows_second, row_count, col_count, chunk, chunks):
    length_first = rows_first * row_count
    length_second = rows_second * col_count
    positions = length_first * length_second
    block = length_first // col_count
    half = block // 2
    a = np.arange(length_first)
    first = np.zeros((col_count, chunks, col_count, block, chunk, row_count, chunk, rows_first))
    for col in range(col_count):
        for i in range(rows_second):
            at, j = divmod(i, chunk)
            p = a * length_second + col * rows_second + i
            for target in range(col_count):
                for f_at in range(half):
                    f = target * half + f_at
                    angle = 2 * np.pi * (f * p % positions) / positions
                    real, imag = np.cos(angle), -np.sin(angle)
                    if f == 0:
                        real, imag = np.ones(length_first), (-1.0) ** a
                    first[col, at, target, 2 * f_at, j, :, j, :] = real.reshape(row_count, rows_first)
                    first[col, at, target, 2 * f_at + 1, j, :, j, :] = imag.reshape(row_count, rows_first)
    first = first.reshape(col_count, chunks, col_count * block * chunk, row_count, chunk * rows_first)
    rest = rows_second - (chunks - 1) * chunk
    last = first[:, -1, :, :, : rest * rows_first].reshape(col_count, col_count * block * chunk, -1)
    first = first.reshape(col_count, chunks, col_count * block * chunk, -1)
    first[:, -1] = 0.0
    first[:, -1, :, : last.shape[-1]] = last
    k_b = np.arange(length_second)
    second = np.zeros((2, 2, length_second, block, col_count, chunks, block, chunk))
    for other in range(2):
        for s in range(block):
            for source in range(col_count):
                for i in range(rows_second):
                    b = source * rows_second + i
                    f_at, upper = s % half, s >= half
                    at, j = divmod(i, chunk)
                    re_at, im_at = (source, at, 2 * f_at, j), (source, at, 2 * f_at + 1, j)
                    if other == 0 and f_at == 0:
                        shift = length_first // 2 if upper else 0
                        angle = 2 * np.pi * (b * (k_b * length_first + shift) % positions) / positions
                        place = im_at if upper else re_at
                        second[(other, 0, slice(None), s) + place] = np.cos(angle)
                        second[(other, 1, slice(None), s) + place] = np.sin(angle)
                        continue
                    sign = -1.0 if upper else 1.0
                    angle = 2 * np.pi * (b * (k_b + (1 if upper else 0)) % length_second) / length_second
                    second[(other, 0, slice(None), s) + re_at] = np.cos(angle)
                    second[(other, 0, slice(None), s) + im_at] = np.sin(angle) * sign
                    second[(other, 1, slice(None), s) + re_at] = np.sin(angle)
                    second[(other, 1, slice(None), s) + im_at] = -np.cos(angle) * sign
    second = second.reshape(2, 2, length_second * block, col_count * chunks * block * chunk)
    return first, second / math.sqrt(positions * GROUP)


def widened(packed, parts, used):
    count, rows, lanes = packed.shape
    flat = packed.reshape(count * rows, lanes).astype(jnp.float32)
    keep = lax.broadcasted_iota(jnp.int32, (1, lanes), 1) < used
    blocks = []
    for p in range(parts):
        block = flat if p == 0 else pltpu.roll(flat, lanes - p * used, 1)
        blocks.append(jnp.where(keep, block, 0.0).astype(packed.dtype).reshape(count, rows, lanes))
    return blocks


def packed_rows(values, parts, used):
    rows = values.shape[0] // parts
    total = values[:rows]
    for p in range(1, parts):
        total = total + pltpu.roll(values[p * rows : (p + 1) * rows], p * used, 1)
    return total


def kernel(
    n_r, n_c, parts, tokens, gain, w_in, forward, first, second, back, out,
    tok_v, gain_v, norm_v, win_v, forward_v, first_v, second_v, back_v,
    sent1, came1, sent2, came2, sent3, came3, wide_v, wide3_v,
    load_sem, self_sem, send_sem1, recv_sem1, send_sem2, recv_sem2, send_sem3, recv_sem3,
):
    row, col = lax.axis_index("row"), lax.axis_index("col")
    rows, features = tokens.shape
    channels = w_in.shape[1]
    tiles = sent1.shape[0]
    span = n_r * GROUP
    spans = [(t * span, min(channels, (t + 1) * span)) for t in range(tiles)]
    width = GROUP // n_r
    used = (spans[-1][1] - spans[-1][0]) // GROUP * width
    order = [tiles - 1] + list(range(tiles - 1))

    barrier = pltpu.get_barrier_semaphore()
    for d in range(1, n_r):
        pl.semaphore_signal(barrier, inc=1, device_id={"row": lax.rem(row + d, n_r)}, device_id_type=MESH)
    for d in range(1, n_c):
        pl.semaphore_signal(barrier, inc=1, device_id={"col": lax.rem(col + d, n_c)}, device_id_type=MESH)

    load_tok = pltpu.make_async_copy(tokens, tok_v, load_sem.at[0])
    load_tok.start()
    load_gain = pltpu.make_async_copy(gain, gain_v, load_sem.at[5])
    load_gain.start()
    load_win = [
        pltpu.make_async_copy(w_in.at[:, lo:hi], win_v.at[:, lo:hi], load_sem.at[6 + t])
        for t, (lo, hi) in enumerate(spans)
    ]
    load_forward = pltpu.make_async_copy(forward, forward_v, load_sem.at[1])
    load_first = pltpu.make_async_copy(first.at[col], first_v, load_sem.at[2])
    load_second = pltpu.make_async_copy(second.at[jnp.minimum(col, 1)], second_v, load_sem.at[3])
    load_back = pltpu.make_async_copy(back, back_v, load_sem.at[4])
    load_win[order[0]].start()
    load_forward.start()
    for t in order[1:]:
        load_win[t].start()
    load_first.start()
    load_second.start()

    load_tok.wait()
    load_gain.wait()
    floats = tok_v[...].astype(jnp.float32)
    inverse = lax.rsqrt(jnp.mean(floats * floats, axis=-1, keepdims=True) + norm_eps)
    gains = gain_v[...].astype(jnp.float32)
    for at in range(features // LANES):
        lanes = slice(at * LANES, (at + 1) * LANES)
        scaled = tok_v[:, lanes].astype(jnp.float32) * inverse * gains[at : at + 1, :]
        norm_v[:, lanes] = scaled.astype(jnp.bfloat16)

    def exchange(sent, came, send_sem, recv_sem, self_sem_at, t, me, count, axis):
        size = sent.shape[2]
        if axis == "row" and t == tiles - 1:
            size = size // parts
        own = pltpu.make_async_copy(sent.at[t, me, 0:size], came.at[t, me, 0:size], self_sem_at)
        copies = []
        for d in sorted(range(1, count), key=lambda d: -min(d, count - d)):
            target = lax.rem(me + d, count)
            copy = pltpu.make_async_remote_copy(
                src_ref=sent.at[t, target, 0:size],
                dst_ref=came.at[t, me, 0:size],
                send_sem=send_sem.at[t, d],
                recv_sem=recv_sem.at[t, d],
                device_id={axis: target},
                device_id_type=MESH,
            )
            copy.start()
            copies.append(copy)
        own.start()
        return [own] + copies

    steps1, steps2, steps3 = {}, {}, {}
    for t in order:
        lo, hi = spans[t]
        load_win[t].wait()
        mapped = jnp.dot(norm_v[...], win_v[:, lo:hi], preferred_element_type=jnp.float32).astype(jnp.bfloat16)
        if t == order[0]:
            load_forward.wait()
        for r in range(n_r):
            piece = jnp.dot(mapped, forward_v[r, : hi - lo, :], preferred_element_type=jnp.float32)
            if t == tiles - 1:
                sent1[t, r, 0 : rows // parts] = packed_rows(piece, parts, used).astype(jnp.bfloat16)
            else:
                sent1[t, r] = piece.astype(jnp.bfloat16)
        if t == order[0]:
            pl.semaphore_wait(barrier, n_r + n_c - 2)
        steps1[t] = exchange(sent1, came1, send_sem1, recv_sem1, self_sem.at[0, t], t, row, n_r, "row")

    load_back.start()
    load_first.wait()
    chunks, high, depth = first_v.shape
    step = depth // n_r
    height = high // n_c
    for t in order:
        for copy in steps1[t]:
            copy.wait()
        source = came1.at[t]
        if t == tiles - 1:
            size = rows // parts
            for p, block in enumerate(widened(came1[t, :, 0:size], parts, used)):
                wide_v[:, p * size : (p + 1) * size] = block
            source = wide_v
        for at in range(chunks):
            values = source[:, at * step : min(rows, (at + 1) * step)]
            values = values.reshape(-1, LANES)
            turned = jnp.dot(first_v[at, :, : values.shape[0]], values, preferred_element_type=jnp.float32)
            turned = turned.astype(jnp.bfloat16).reshape(n_c, height, LANES)
            sent2[t, :, at * height : (at + 1) * height] = turned
        steps2[t] = exchange(sent2, came2, send_sem2, recv_sem2, self_sem.at[1, t], t, col, n_c, "col")

    lane = lax.broadcasted_iota(jnp.int32, (1, LANES), 1) % width
    cosine = (lane < width // 2) | ((lane == width // 2) & (row == 0))
    load_second.wait()
    out_rows = sent3.shape[2]
    for t in order:
        for copy in steps2[t]:
            copy.wait()
        values = came2[t].reshape(-1, LANES)
        even = jnp.dot(second_v[0], values, preferred_element_type=jnp.float32)
        odd = jnp.dot(second_v[1], values, preferred_element_type=jnp.float32)
        both = jnp.where(cosine, even, odd)
        if t == tiles - 1:
            for r in range(n_r):
                block = packed_rows(both[r * out_rows : (r + 1) * out_rows], parts, used)
                sent3[t, r, 0 : out_rows // parts] = block.astype(jnp.bfloat16)
        else:
            sent3[t] = both.astype(jnp.bfloat16).reshape(sent3.shape[1:])
        steps3[t] = exchange(sent3, came3, send_sem3, recv_sem3, self_sem.at[2, t], t, row, n_r, "row")

    load_back.wait()
    for t in order:
        lo, hi = spans[t]
        for copy in steps3[t]:
            copy.wait()
        source = came3.at[t]
        if t == tiles - 1:
            size = out_rows // parts
            for p, block in enumerate(widened(came3[t, :, 0:size], parts, used)):
                wide3_v[:, p * size : (p + 1) * size] = block
            source = wide3_v
        total = jnp.dot(source[0], back_v[0, :, : hi - lo], preferred_element_type=jnp.float32)
        for r in range(1, n_r):
            total = total + jnp.dot(source[r], back_v[r, :, : hi - lo], preferred_element_type=jnp.float32)
        out[:, lo:hi] = total.astype(jnp.bfloat16)


def last_product(spectrum, w_out, out):
    total = jnp.dot(spectrum[...], w_out[...], preferred_element_type=jnp.float32)
    out[...] = total.reshape(out.shape).astype(jnp.bfloat16)


def fused_shards(n_r, n_c, tokens, norm_gain, w_in, w_out):
    rows_first, rows_second, features = tokens.shape
    channels = w_in.shape[1]
    length_first = rows_first * n_r
    block = length_first // n_c
    chunk = SUBLANES // block
    chunks = -(-rows_second // chunk)
    padded = chunks * SUBLANES
    groups = channels // GROUP
    tiles = -(-groups // n_r)
    rows = rows_first * rows_second
    length_second = rows_second * n_c
    out_rows = length_second // n_r * block
    forward, back = channel_tables(n_r)
    first, second = position_tables(rows_first, rows_second, n_r, n_c, chunk, chunks)
    used = (groups - (tiles - 1) * n_r) * (GROUP // n_r)
    parts = max(p for p in range(1, LANES // used + 1) if rows % (SUBLANES * p) == 0 and out_rows % (SUBLANES * p) == 0)
    tokens = tokens.transpose(1, 0, 2).reshape(rows, features)
    kind = jnp.bfloat16
    tables = [jnp.asarray(np.asarray(x, np.float32).astype(kind)) for x in (forward, first, second, back)]
    hbm = pl.BlockSpec(memory_space=pltpu.HBM)
    vmem = pl.BlockSpec(memory_space=pltpu.VMEM)
    dma = pltpu.SemaphoreType.DMA
    spectrum = pl.pallas_call(
        functools.partial(kernel, n_r, n_c, parts),
        out_shape=pltpu.VMEM((out_rows, channels), kind),
        in_specs=[hbm] * 7,
        out_specs=vmem,
        scratch_shapes=[
            pltpu.VMEM(tokens.shape, kind),
            pltpu.VMEM((features // LANES, LANES), kind),
            pltpu.VMEM((rows, features), kind),
            pltpu.VMEM(w_in.shape, kind),
            pltpu.VMEM(forward.shape, kind),
            pltpu.VMEM(first.shape[1:], kind),
            pltpu.VMEM(second.shape[1:], kind),
            pltpu.VMEM(back.shape, kind),
            pltpu.VMEM((tiles, n_r, rows, LANES), kind),
            pltpu.VMEM((tiles, n_r, rows, LANES), kind),
            pltpu.VMEM((tiles, n_c, padded, LANES), kind),
            pltpu.VMEM((tiles, n_c, padded, LANES), kind),
            pltpu.VMEM((tiles, n_r, out_rows, LANES), kind),
            pltpu.VMEM((tiles, n_r, out_rows, LANES), kind),
            pltpu.VMEM((n_r, rows, LANES), kind),
            pltpu.VMEM((n_r, out_rows, LANES), kind),
            dma((6 + tiles,)),
            dma((3, tiles)),
            dma((tiles, n_r)),
            dma((tiles, n_r)),
            dma((tiles, n_c)),
            dma((tiles, n_c)),
            dma((tiles, n_r)),
            dma((tiles, n_r)),
        ],
        compiler_params=pltpu.CompilerParams(
            collective_id=0, has_side_effects=True, vmem_limit_bytes=53 * 1024 * 1024
        ),
    )(*[pltpu.with_memory_space_constraint(x, pltpu.HBM) for x in (tokens, norm_gain.reshape(-1, LANES), w_in, *tables)])
    return pl.pallas_call(
        last_product,
        out_shape=jax.ShapeDtypeStruct((length_second // n_r, block, features), kind),
        in_specs=[vmem] * 2,
        out_specs=vmem,
        compiler_params=pltpu.CompilerParams(vmem_limit_bytes=16 * 1024 * 1024),
    )(spectrum, w_out)


def fits(n_r, n_c, tokens_shape, channels):
    length_first, length_second, _ = tokens_shape
    rows = length_first // n_r * (length_second // n_c)
    out_rows = length_second // n_r * (length_first // n_c)
    return (
        GROUP % (2 * n_r) == 0
        and length_first % (2 * n_c) == 0
        and SUBLANES % (length_first // n_c) == 0
        and rows % SUBLANES == 0
        and out_rows % SUBLANES == 0
        and length_first // n_r * (SUBLANES // (length_first // n_c)) % SUBLANES == 0
        and length_second % n_r == 0
    )


def tables(length):
    series = jnp.arange(length, dtype=jnp.int32)
    product = series[:, None] * series[None, :] % length
    angles = product.astype(jnp.float32) * (2.0 * math.pi / length)
    return (jnp.cos(angles), jnp.sin(angles))


def folded_order(length_first, devices):
    block = length_first // devices
    half_block = block // 2
    series = jnp.arange(length_first, dtype=jnp.int32)
    device = series // block
    inner = series % block
    lower = device * half_block + inner
    upper = length_first - device * half_block - (inner - half_block)
    upper = jnp.where((device == 0) & (inner == half_block), length_first // 2, upper)
    return jnp.where(inner < half_block, lower, upper) % length_first


def to_channels(values, row_count):
    rows_first, rows_second, channels = values.shape
    width = channels // row_count
    parted = values.reshape(rows_first, rows_second, row_count, width).transpose(2, 0, 1, 3)
    return parted.reshape(row_count * rows_first, rows_second * width)


def product(table, values):
    return jnp.dot(table, values, precision=highest)


def middle(real_part, imag_part, width):
    length_first = real_part.shape[0]
    rows_second = real_part.shape[1] // width
    col_count = lax.axis_size("col")
    length_second = rows_second * col_count
    positions = length_first * length_second
    frequency = folded_order(length_first, col_count)
    series = jnp.arange(length_first, dtype=jnp.int32)
    first_angle = (frequency[:, None] * series[None, :] % length_first).astype(jnp.float32)
    first_angle = first_angle * (2.0 * math.pi / length_first)
    first_cos = jnp.cos(first_angle)
    first_sin = jnp.sin(first_angle)
    first_real = product(first_cos, real_part)
    first_imag = -product(first_sin, real_part)
    first_real = first_real + product(first_sin, imag_part)
    first_imag = first_imag + product(first_cos, imag_part)
    first_real = first_real.reshape(length_first, rows_second, width)
    first_imag = first_imag.reshape(length_first, rows_second, width)
    second_index = lax.axis_index("col") * rows_second + jnp.arange(rows_second, dtype=jnp.int32)
    twiddle_angle = (frequency[:, None] * second_index[None, :] % positions).astype(jnp.float32)
    twiddle_angle = twiddle_angle * (2.0 * math.pi / positions)
    twiddle_cos = jnp.cos(twiddle_angle)[:, :, None]
    twiddle_sin = jnp.sin(twiddle_angle)[:, :, None]
    turned_real = first_real * twiddle_cos + first_imag * twiddle_sin
    turned_imag = first_imag * twiddle_cos - first_real * twiddle_sin
    turned = jnp.stack([turned_real, turned_imag]).transpose(0, 2, 1, 3)
    turned = turned.reshape(2, rows_second, length_first * width)
    exchanged = lax.all_to_all(
        turned.astype(jnp.bfloat16), "col", split_axis=2, concat_axis=1, tiled=True
    ).astype(turned.dtype)
    second_cos, second_sin = tables(length_second)
    block = length_first // col_count
    out_shape = (length_second, block, width)
    out_real = (product(second_cos, exchanged[0]) + product(second_sin, exchanged[1])).reshape(
        out_shape
    )
    return out_real


def shards(tokens, norm_gain, w_in, w_out):
    rows_first, rows_second, features = tokens.shape
    row_count = lax.axis_size("row")
    length_first = rows_first * row_count
    length_second = rows_second * lax.axis_size("col")
    channels = w_in.shape[1]
    width = channels // row_count
    groups = channels // GROUP
    scaling = 1.0 / math.sqrt(length_first * length_second * GROUP)
    floats = tokens.astype(jnp.float32)
    normed = (
        floats
        * lax.rsqrt(jnp.mean(floats * floats, axis=-1, keepdims=True) + norm_eps)
        * norm_gain.astype(jnp.float32)
    ).astype(jnp.bfloat16)
    mapped = jnp.dot(normed.reshape(-1, features), w_in, preferred_element_type=jnp.float32)
    mapped = mapped.astype(jnp.bfloat16).reshape(rows_first, rows_second, channels)
    channel_cos, channel_sin = tables(GROUP)
    grouped = mapped.astype(jnp.float32).reshape(rows_first, rows_second, groups, GROUP)
    spec_real = jnp.einsum("abgj,jm->abgm", grouped, channel_cos, precision=highest)
    spec_imag = -jnp.einsum("abgj,jm->abgm", grouped, channel_sin, precision=highest)
    stacked = jnp.stack(
        [
            to_channels(spec_real.reshape(rows_first, rows_second, channels), row_count),
            to_channels(spec_imag.reshape(rows_first, rows_second, channels), row_count),
        ]
    )
    arrived = lax.all_to_all(
        stacked.astype(jnp.bfloat16), "row", split_axis=1, concat_axis=1, tiled=True
    ).astype(stacked.dtype)
    result = middle(arrived[0], arrived[1], width)
    spectrum = (result * scaling).astype(jnp.bfloat16)
    returned = lax.all_to_all(spectrum, "row", split_axis=0, concat_axis=2, tiled=True)
    mixed = jnp.dot(returned.reshape(-1, channels), w_out, preferred_element_type=jnp.float32)
    return mixed.astype(jnp.bfloat16).reshape(returned.shape[0], returned.shape[1], features)


def solution(mesh):
    in_specs = (P("row", "col", None), P(), P(), P())
    out_specs = P("row", "col", None)
    n_r, n_c = mesh.shape["row"], mesh.shape["col"]

    def run(tokens, norm_gain, w_in, w_out):
        whole = fits(n_r, n_c, tokens.shape, w_in.shape[1])
        body = functools.partial(fused_shards, n_r, n_c) if whole else shards
        return jax.shard_map(body, mesh=mesh, in_specs=in_specs, out_specs=out_specs, check_vma=False)(
            tokens, norm_gain, w_in, w_out
        )

    return run
```

```python
import functools
import math

import jax
import jax.numpy as jnp
import numpy as np
from jax import lax
from jax.experimental import pallas as pl
from jax.experimental.pallas import tpu as pltpu
from jax.sharding import PartitionSpec as P

GROUP = 128
LANES = 128
SUBLANES = 16
ROWS = 8
LAG = 2
MESH = pl.DeviceIdType.MESH


norm_eps = 1e-06
highest = lax.Precision.HIGHEST


def folded_list(length_first, devices):
    block = length_first // devices
    half = block // 2
    result = np.zeros(length_first, np.int64)
    for device in range(devices):
        for inner in range(block):
            if inner < half:
                value = device * half + inner
            elif device == 0 and inner == half:
                value = length_first // 2
            else:
                value = length_first - device * half - (inner - half)
            result[device * block + inner] = value % length_first
    return result


def ceil_to(value, multiple):
    return -(-value // multiple) * multiple


class Piece:
    def __init__(self, groups, n_r, n_c, rows_first, rows_second, length_second):
        self.groups = groups
        self.channels = groups * GROUP
        self.used = groups * GROUP // n_r
        self.parts = LANES // self.used
        self.seconds = -(-rows_second // self.parts)
        self.block = rows_first * n_r // n_c
        self.rows1 = self.seconds * rows_first
        self.rows2 = ceil_to(self.seconds * self.block, ROWS)
        self.out_rows = length_second // n_r * self.block
        self.rows3 = ceil_to(-(-self.out_rows // self.parts), ROWS)


def chunk_sizes(groups, n_r):
    per = LANES // 2 // (GROUP // n_r)
    rest = groups % per
    return [per] * (groups // per) + ([rest] if rest else [])


def channel_tables(piece, n_r):
    width = GROUP // n_r
    half = width // 2
    j = np.arange(GROUP)
    forward = np.zeros((piece.parts, piece.groups, GROUP, n_r, piece.parts, piece.groups, width))
    back = np.zeros((n_r, piece.parts, piece.groups, width, piece.parts, piece.groups, GROUP))
    for row in range(n_r):
        for x in range(width):
            m = row * half + x % half
            cosine = x < half
            column = np.cos(2 * np.pi * j * m / GROUP) if cosine else np.sin(2 * np.pi * j * m / GROUP)
            entries = [(m, 1.0)]
            if not cosine and m == 0:
                column = np.cos(np.pi * j)
                entries = [(GROUP // 2, 1.0)]
            elif m:
                entries = [(m, 1.0 if cosine else -1.0), (GROUP - m, 1.0)]
            for q in range(piece.parts):
                for g in range(piece.groups):
                    forward[q, g, :, row, q, g, x] = column
                    for at, sign in entries:
                        back[row, q, g, x, q, g, at] = sign
    size = piece.parts * piece.channels
    return forward.reshape(size, n_r * LANES), back.reshape(n_r * LANES, size)


def position_tables(piece, rows_first, rows_second, n_r, n_c):
    length_first = rows_first * n_r
    length_second = rows_second * n_c
    positions = length_first * length_second
    block, parts, seconds = piece.block, piece.parts, piece.seconds
    half = block // 2
    a = np.arange(length_first)
    first = np.zeros((n_c, parts, n_c, piece.rows2, n_r, seconds, rows_first))
    for col in range(n_c):
        for i in range(rows_second):
            q, j = divmod(i, seconds)
            p = a * length_second + col * rows_second + i
            for target in range(n_c):
                for f_at in range(half):
                    f = target * half + f_at
                    angle = 2 * np.pi * (f * p % positions) / positions
                    real, imag = np.cos(angle), -np.sin(angle)
                    if f == 0:
                        real, imag = np.ones(length_first), (-1.0) ** a
                    first[col, q, target, j * block + 2 * f_at, :, j, :] = real.reshape(n_r, rows_first)
                    first[col, q, target, j * block + 2 * f_at + 1, :, j, :] = imag.reshape(n_r, rows_first)
    k_b = np.arange(length_second)
    plain = np.zeros((2, 2, length_second, block, parts, n_c, piece.rows2))
    for other in range(2):
        for s in range(block):
            for source in range(n_c):
                for i in range(rows_second):
                    b = source * rows_second + i
                    f_at, upper = s % half, s >= half
                    q, j = divmod(i, seconds)
                    re_at, im_at = (q, source, j * block + 2 * f_at), (q, source, j * block + 2 * f_at + 1)
                    if other == 0 and f_at == 0:
                        shift = length_first // 2 if upper else 0
                        angle = 2 * np.pi * (b * (k_b * length_first + shift) % positions) / positions
                        place = im_at if upper else re_at
                        plain[(other, 0, slice(None), s) + place] = np.cos(angle)
                        plain[(other, 1, slice(None), s) + place] = np.sin(angle)
                        continue
                    sign = -1.0 if upper else 1.0
                    angle = 2 * np.pi * (b * (k_b + (1 if upper else 0)) % length_second) / length_second
                    plain[(other, 0, slice(None), s) + re_at] = np.cos(angle)
                    plain[(other, 0, slice(None), s) + im_at] = np.sin(angle) * sign
                    plain[(other, 1, slice(None), s) + re_at] = np.sin(angle)
                    plain[(other, 1, slice(None), s) + im_at] = -np.cos(angle) * sign
    plain = plain.reshape(2, 2, n_r, piece.out_rows, parts, n_c * piece.rows2) / math.sqrt(positions * GROUP)
    second = np.zeros((2, n_r, parts, 2, piece.rows3, parts, n_c * piece.rows2))
    for q in range(parts):
        lo, hi = q * piece.rows3, min(piece.out_rows, (q + 1) * piece.rows3)
        for d in range(parts):
            values = plain[:, :, :, lo:hi, (q - d) % parts]
            second[:, :, q, :, : hi - lo, d] = values.transpose(0, 2, 1, 3, 4)
    first = first.reshape(n_c, parts * n_c * piece.rows2, n_r * piece.rows1)
    return first, second.reshape(2, n_r, parts * 2 * piece.rows3, parts * n_c * piece.rows2)


def bits_apart(one, other, count):
    total, bit = 0, 1
    while bit < count:
        total = total + bit * ((one // bit + other // bit) % 2)
        bit *= 2
    return total


def far_first(me, count):
    places = []
    for k in range(count - 1):
        down = count - 1 - k - jnp.where(count - 1 - k <= me, 1, 0)
        up = k + jnp.where(k >= me, 1, 0)
        places.append(jnp.where(me < count // 2, down, up))
    return places


def kernel(n_r, n_c, pieces, kinds, *refs):
    refs = list(refs)

    def take(count):
        taken = refs[:count]
        del refs[:count]
        return taken

    many = len(pieces)
    tokens, gain, w_in = take(3)
    tables_hbm = [take(4) for _ in pieces]
    (out,) = take(1)
    tok_v, gain_v, norm_v, win_v = take(4)
    tables_v = [take(4) for _ in pieces]
    buffers = [take(6) for _ in pieces]
    load_sem, table_sem, self_sem, send1, recv1, send2, recv2, send3, recv3 = take(9)
    row, col = lax.axis_index("row"), lax.axis_index("col")
    rows, features = tokens.shape
    steps = len(kinds)
    spans, seats = [], []
    lo = 0
    for at, kind in enumerate(kinds):
        spans.append((lo, lo + pieces[kind].channels))
        seats.append(kinds[:at].count(kind))
        lo = spans[-1][1]

    barrier = pltpu.get_barrier_semaphore()
    for d in range(1, n_r):
        pl.semaphore_signal(barrier, inc=1, device_id={"row": bits_apart(row, d, n_r)}, device_id_type=MESH)
    for d in range(1, n_c):
        pl.semaphore_signal(barrier, inc=1, device_id={"col": bits_apart(col, d, n_c)}, device_id_type=MESH)

    load_tok = pltpu.make_async_copy(tokens, tok_v, load_sem.at[0])
    load_gain = pltpu.make_async_copy(gain, gain_v, load_sem.at[1])
    load_win = [
        pltpu.make_async_copy(w_in.at[:, lo:hi], win_v.at[:, lo:hi], load_sem.at[2 + t])
        for t, (lo, hi) in enumerate(spans)
    ]
    load = []
    for p, (forward, first, second, back) in enumerate(tables_hbm):
        sources = (forward, first.at[col], second.at[jnp.minimum(col, 1)], back)
        load.append(
            [pltpu.make_async_copy(x, y, table_sem.at[p, n]) for n, (x, y) in enumerate(zip(sources, tables_v[p]))]
        )
    load_tok.start()
    load_gain.start()
    started = set()
    for t, kind in enumerate(kinds):
        load_win[t].start()
        if kind not in started:
            load[kind][0].start()
            started.add(kind)
    for n in (1, 2):
        for p in range(many):
            load[p][n].start()
    pending = {(p, n) for p in range(many) for n in range(4)}

    def table(p, n):
        if (p, n) in pending:
            load[p][n].wait()
            pending.discard((p, n))
        return tables_v[p][n]

    load_tok.wait()
    load_gain.wait()
    floats = tok_v[...].astype(jnp.float32)
    inverse = lax.rsqrt(jnp.mean(floats * floats, axis=-1, keepdims=True) + norm_eps)
    gains = gain_v[...].astype(jnp.float32)
    for at in range(features // LANES):
        lanes = slice(at * LANES, (at + 1) * LANES)
        scaled = tok_v[:, lanes].astype(jnp.float32) * inverse * gains[at : at + 1, :]
        norm_v[:, lanes] = scaled.astype(jnp.bfloat16)

    row_targets = far_first(row, n_r)
    col_targets = [bits_apart(col, d, n_c) for d in range(n_c - 1, 0, -1)]
    stages = (
        (row, row_targets, send1, recv1, "row"),
        (col, col_targets, send2, recv2, "col"),
        (row, row_targets, send3, recv3, "row"),
    )

    def send(sent, came, stage, seat, t, target):
        me, targets, send_sem, recv_sem, axis = stages[stage]
        d = bits_apart(me, target, len(targets) + 1)
        copy = pltpu.make_async_remote_copy(
            src_ref=sent.at[seat, target],
            dst_ref=came.at[seat, me],
            send_sem=send_sem.at[t, d],
            recv_sem=recv_sem.at[t, d],
            device_id={axis: target},
            device_id_type=MESH,
        )
        copy.start()
        return copy

    def keep(sent, came, stage, seat, t):
        me = stages[stage][0]
        copy = pltpu.make_async_copy(sent.at[seat, me], came.at[seat, me], self_sem.at[stage, t])
        copy.start()
        return copy

    def exchange(sent, came, stage, seat, t):
        copies = [send(sent, came, stage, seat, t, target) for target in stages[stage][1]]
        return copies + [keep(sent, came, stage, seat, t)]

    lane = lax.broadcasted_iota(jnp.int32, (1, LANES), 1)
    turn = lane % (GROUP // n_r)
    cosine = (turn < GROUP // n_r // 2) | ((turn == GROUP // n_r // 2) & (row == 0))
    copies1, copies2, copies3 = {}, {}, {}

    def start(t):
        p, seat = kinds[t], seats[t]
        piece = pieces[p]
        lo, hi = spans[t]
        load_win[t].wait()
        mapped = jnp.dot(norm_v[...], win_v[:, lo:hi], preferred_element_type=jnp.float32)
        short = piece.parts * piece.rows1 - rows
        if short:
            mapped = jnp.concatenate([mapped, jnp.zeros((short, hi - lo), jnp.float32)], axis=0)
        blocks = [mapped[q * piece.rows1 : (q + 1) * piece.rows1] for q in range(piece.parts)]
        side = jnp.concatenate(blocks, axis=1).astype(jnp.bfloat16)
        turned = jnp.dot(side, table(p, 0)[...], preferred_element_type=jnp.float32).astype(jnp.bfloat16)
        sent, came = buffers[p][:2]
        for r in range(n_r):
            sent[seat, r] = turned[:, r * LANES : (r + 1) * LANES]
        if t == 0:
            pl.semaphore_wait(barrier, n_r + n_c - 2)
        copies1[t] = exchange(sent, came, 0, seat, t)

    def middle_first(t):
        p, seat = kinds[t], seats[t]
        piece = pieces[p]
        weights = table(p, 1)
        for copy in copies1[t]:
            copy.wait()
        values = buffers[p][1][seat].reshape(n_r * piece.rows1, LANES)
        both = jnp.dot(weights[...], values, preferred_element_type=jnp.float32)
        size = n_c * piece.rows2
        total = both[:size]
        for q in range(1, piece.parts):
            total = jnp.where(lane < q * piece.used, total, both[q * size : (q + 1) * size])
        sent, came = buffers[p][2:4]
        sent[seat] = total.astype(jnp.bfloat16).reshape(n_c, piece.rows2, LANES)
        copies2[t] = exchange(sent, came, 1, seat, t)

    def middle_second(t):
        p, seat = kinds[t], seats[t]
        piece = pieces[p]
        weights = table(p, 2)
        for copy in copies2[t]:
            copy.wait()
        values = buffers[p][3][seat].reshape(n_c * piece.rows2, LANES)
        floats = values.astype(jnp.float32)
        rolled = [values] + [
            pltpu.roll(floats, d * piece.used, 1).astype(jnp.bfloat16) for d in range(1, piece.parts)
        ]
        deep = jnp.concatenate(rolled, axis=0)
        sent, came = buffers[p][4:6]
        size = piece.rows3
        for r in range(n_r):
            both = jnp.dot(weights[r], deep, preferred_element_type=jnp.float32)
            chosen = [
                jnp.where(cosine, both[2 * q * size : (2 * q + 1) * size], both[(2 * q + 1) * size : (2 * q + 2) * size])
                for q in range(piece.parts)
            ]
            total = chosen[0]
            for q in range(1, piece.parts):
                total = jnp.where(lane < q * piece.used, total, chosen[q])
            sent[seat, r] = total.astype(jnp.bfloat16)
        copies3[t] = exchange(sent, came, 2, seat, t)

    def finish(t):
        p, seat = kinds[t], seats[t]
        piece = pieces[p]
        lo, hi = spans[t]
        weights = table(p, 3)
        for copy in copies3[t]:
            copy.wait()
        side = jnp.concatenate([buffers[p][5][seat, r] for r in range(n_r)], axis=1)
        total = jnp.dot(side, weights[...], preferred_element_type=jnp.float32).astype(jnp.bfloat16)
        size = piece.channels
        for q in range(piece.parts):
            above, below = q * piece.rows3, min(piece.out_rows, (q + 1) * piece.rows3)
            out[above:below, lo:hi] = total[: below - above, q * size : (q + 1) * size]

    for t in range(steps):
        start(t)
    for p in range(many):
        load[p][3].start()
    for job, t in schedule(steps):
        (middle_first, middle_second, finish)[job](t)


def schedule(steps):
    jobs, ready = [], 0
    for t in range(steps):
        jobs.append((0, t))
        while ready <= t - LAG:
            jobs.append((1, ready))
            ready += 1
    jobs += [(1, t) for t in range(ready, steps)]
    return jobs + [(2, t) for t in range(steps)]


def last_product(spectrum, w_out, out):
    total = jnp.dot(spectrum[...], w_out[...], preferred_element_type=jnp.float32)
    out[...] = total.reshape(out.shape).astype(jnp.bfloat16)


def fused_shards(n_r, n_c, tokens, norm_gain, w_in, w_out):
    rows_first, rows_second, features = tokens.shape
    channels = w_in.shape[1]
    length_second = rows_second * n_c
    sizes = chunk_sizes(channels // GROUP, n_r)
    distinct = sorted(set(sizes))
    kinds = [distinct.index(size) for size in sizes]
    pieces = [Piece(size, n_r, n_c, rows_first, rows_second, length_second) for size in distinct]
    block, out_rows = pieces[0].block, pieces[0].out_rows
    rows = rows_first * rows_second
    tokens = tokens.transpose(1, 0, 2).reshape(rows, features)
    kind = jnp.bfloat16
    tables = []
    for piece in pieces:
        forward, back = channel_tables(piece, n_r)
        first, second = position_tables(piece, rows_first, rows_second, n_r, n_c)
        tables += [jnp.asarray(np.asarray(x, np.float32).astype(kind)) for x in (forward, first, second, back)]
    hbm = pl.BlockSpec(memory_space=pltpu.HBM)
    vmem = pl.BlockSpec(memory_space=pltpu.VMEM)
    dma = pltpu.SemaphoreType.DMA
    scratch = [
        pltpu.VMEM((rows, features), kind),
        pltpu.VMEM((features // LANES, LANES), kind),
        pltpu.VMEM((rows, features), kind),
        pltpu.VMEM(w_in.shape, kind),
    ]
    for p in range(len(pieces)):
        forward, first, second, back = tables[4 * p : 4 * p + 4]
        scratch += [pltpu.VMEM(x, kind) for x in (forward.shape, first.shape[1:], second.shape[1:], back.shape)]
    for p, piece in enumerate(pieces):
        count = kinds.count(p)
        for first_size, second_size in ((n_r, piece.rows1), (n_c, piece.rows2), (n_r, piece.rows3)):
            scratch += [pltpu.VMEM((count, first_size, second_size, LANES), kind)] * 2
    steps = len(kinds)
    scratch += [dma((2 + steps,)), dma((len(pieces), 4)), dma((3, steps))]
    scratch += [dma((steps, n)) for n in (n_r, n_r, n_c, n_c, n_r, n_r)]
    operands = (tokens, norm_gain.reshape(-1, LANES), w_in, *tables)
    spectrum = pl.pallas_call(
        functools.partial(kernel, n_r, n_c, pieces, kinds),
        out_shape=pltpu.VMEM((out_rows, channels), kind),
        in_specs=[hbm] * len(operands),
        out_specs=vmem,
        scratch_shapes=scratch,
        compiler_params=pltpu.CompilerParams(
            collective_id=0, has_side_effects=True, vmem_limit_bytes=53 * 1024 * 1024
        ),
    )(*[pltpu.with_memory_space_constraint(x, pltpu.HBM) for x in operands])
    return pl.pallas_call(
        last_product,
        out_shape=jax.ShapeDtypeStruct((length_second // n_r, block, features), kind),
        in_specs=[vmem] * 2,
        out_specs=vmem,
        compiler_params=pltpu.CompilerParams(vmem_limit_bytes=16 * 1024 * 1024),
    )(spectrum, w_out)


def fits(n_r, n_c, tokens_shape, channels):
    length_first, length_second, _ = tokens_shape
    return (
        n_r > 1
        and n_c & (n_c - 1) == 0
        and GROUP % (2 * n_r) == 0
        and length_first % (2 * n_c) == 0
        and SUBLANES % (length_first // n_c) == 0
        and length_first // n_r % ROWS == 0
        and length_second // n_r * (length_first // n_c) % ROWS == 0
        and length_second % n_r == 0
        and all(LANES % (size * GROUP // n_r) == 0 for size in chunk_sizes(channels // GROUP, n_r))
    )


def tables(length):
    series = jnp.arange(length, dtype=jnp.int32)
    product = series[:, None] * series[None, :] % length
    angles = product.astype(jnp.float32) * (2.0 * math.pi / length)
    return (jnp.cos(angles), jnp.sin(angles))


def folded_order(length_first, devices):
    block = length_first // devices
    half_block = block // 2
    series = jnp.arange(length_first, dtype=jnp.int32)
    device = series // block
    inner = series % block
    lower = device * half_block + inner
    upper = length_first - device * half_block - (inner - half_block)
    upper = jnp.where((device == 0) & (inner == half_block), length_first // 2, upper)
    return jnp.where(inner < half_block, lower, upper) % length_first


def to_channels(values, row_count):
    rows_first, rows_second, channels = values.shape
    width = channels // row_count
    parted = values.reshape(rows_first, rows_second, row_count, width).transpose(2, 0, 1, 3)
    return parted.reshape(row_count * rows_first, rows_second * width)


def product(table, values):
    return jnp.dot(table, values, precision=highest)


def middle(real_part, imag_part, width):
    length_first = real_part.shape[0]
    rows_second = real_part.shape[1] // width
    col_count = lax.axis_size("col")
    length_second = rows_second * col_count
    positions = length_first * length_second
    frequency = folded_order(length_first, col_count)
    series = jnp.arange(length_first, dtype=jnp.int32)
    first_angle = (frequency[:, None] * series[None, :] % length_first).astype(jnp.float32)
    first_angle = first_angle * (2.0 * math.pi / length_first)
    first_cos = jnp.cos(first_angle)
    first_sin = jnp.sin(first_angle)
    first_real = product(first_cos, real_part)
    first_imag = -product(first_sin, real_part)
    first_real = first_real + product(first_sin, imag_part)
    first_imag = first_imag + product(first_cos, imag_part)
    first_real = first_real.reshape(length_first, rows_second, width)
    first_imag = first_imag.reshape(length_first, rows_second, width)
    second_index = lax.axis_index("col") * rows_second + jnp.arange(rows_second, dtype=jnp.int32)
    twiddle_angle = (frequency[:, None] * second_index[None, :] % positions).astype(jnp.float32)
    twiddle_angle = twiddle_angle * (2.0 * math.pi / positions)
    twiddle_cos = jnp.cos(twiddle_angle)[:, :, None]
    twiddle_sin = jnp.sin(twiddle_angle)[:, :, None]
    turned_real = first_real * twiddle_cos + first_imag * twiddle_sin
    turned_imag = first_imag * twiddle_cos - first_real * twiddle_sin
    turned = jnp.stack([turned_real, turned_imag]).transpose(0, 2, 1, 3)
    turned = turned.reshape(2, rows_second, length_first * width)
    exchanged = lax.all_to_all(
        turned.astype(jnp.bfloat16), "col", split_axis=2, concat_axis=1, tiled=True
    ).astype(turned.dtype)
    second_cos, second_sin = tables(length_second)
    block = length_first // col_count
    out_shape = (length_second, block, width)
    out_real = (product(second_cos, exchanged[0]) + product(second_sin, exchanged[1])).reshape(
        out_shape
    )
    return out_real


def shards(tokens, norm_gain, w_in, w_out):
    rows_first, rows_second, features = tokens.shape
    row_count = lax.axis_size("row")
    length_first = rows_first * row_count
    length_second = rows_second * lax.axis_size("col")
    channels = w_in.shape[1]
    width = channels // row_count
    groups = channels // GROUP
    scaling = 1.0 / math.sqrt(length_first * length_second * GROUP)
    floats = tokens.astype(jnp.float32)
    normed = (
        floats
        * lax.rsqrt(jnp.mean(floats * floats, axis=-1, keepdims=True) + norm_eps)
        * norm_gain.astype(jnp.float32)
    ).astype(jnp.bfloat16)
    mapped = jnp.dot(normed.reshape(-1, features), w_in, preferred_element_type=jnp.float32)
    mapped = mapped.astype(jnp.bfloat16).reshape(rows_first, rows_second, channels)
    channel_cos, channel_sin = tables(GROUP)
    grouped = mapped.astype(jnp.float32).reshape(rows_first, rows_second, groups, GROUP)
    spec_real = jnp.einsum("abgj,jm->abgm", grouped, channel_cos, precision=highest)
    spec_imag = -jnp.einsum("abgj,jm->abgm", grouped, channel_sin, precision=highest)
    stacked = jnp.stack(
        [
            to_channels(spec_real.reshape(rows_first, rows_second, channels), row_count),
            to_channels(spec_imag.reshape(rows_first, rows_second, channels), row_count),
        ]
    )
    arrived = lax.all_to_all(
        stacked.astype(jnp.bfloat16), "row", split_axis=1, concat_axis=1, tiled=True
    ).astype(stacked.dtype)
    result = middle(arrived[0], arrived[1], width)
    spectrum = (result * scaling).astype(jnp.bfloat16)
    returned = lax.all_to_all(spectrum, "row", split_axis=0, concat_axis=2, tiled=True)
    mixed = jnp.dot(returned.reshape(-1, channels), w_out, preferred_element_type=jnp.float32)
    return mixed.astype(jnp.bfloat16).reshape(returned.shape[0], returned.shape[1], features)


def solution(mesh):
    in_specs = (P("row", "col", None), P(), P(), P())
    out_specs = P("row", "col", None)
    n_r, n_c = mesh.shape["row"], mesh.shape["col"]

    def run(tokens, norm_gain, w_in, w_out):
        whole = fits(n_r, n_c, tokens.shape, w_in.shape[1])
        body = functools.partial(fused_shards, n_r, n_c) if whole else shards
        return jax.shard_map(body, mesh=mesh, in_specs=in_specs, out_specs=out_specs, check_vma=False)(
            tokens, norm_gain, w_in, w_out
        )

    return run
```

```python
import functools
import math

import jax
import jax.numpy as jnp
import numpy as np
from jax import lax
from jax.experimental import pallas as pl
from jax.experimental.pallas import tpu as pltpu
from jax.sharding import PartitionSpec as P

GROUP = 128
LANES = 128
SUBLANES = 16
ROWS = 8
LAG = 3
TAIL = 2
HELD = 3
COLUMNS = 512
MESH = pl.DeviceIdType.MESH


norm_eps = 1e-06
highest = lax.Precision.HIGHEST


def folded_list(length_first, devices):
    block = length_first // devices
    half = block // 2
    result = np.zeros(length_first, np.int64)
    for device in range(devices):
        for inner in range(block):
            if inner < half:
                value = device * half + inner
            elif device == 0 and inner == half:
                value = length_first // 2
            else:
                value = length_first - device * half - (inner - half)
            result[device * block + inner] = value % length_first
    return result


def ceil_to(value, multiple):
    return -(-value // multiple) * multiple


class Piece:
    def __init__(self, groups, n_r, n_c, rows_first, rows_second, length_second):
        self.groups = groups
        self.channels = groups * GROUP
        self.used = groups * GROUP // n_r
        self.parts = LANES // self.used
        self.seconds = -(-rows_second // self.parts)
        self.block = rows_first * n_r // n_c
        self.rows1 = self.seconds * rows_first
        self.rows2 = ceil_to(self.seconds * self.block, ROWS)
        self.out_rows = length_second // n_r * self.block
        self.rows3 = ceil_to(-(-self.out_rows // self.parts), ROWS)


def chunk_sizes(groups, n_r):
    per = LANES // 2 // (GROUP // n_r)
    rest = groups % per
    return [per] * (groups // per) + ([rest] if rest else [])


def channel_tables(piece, n_r):
    width = GROUP // n_r
    half = width // 2
    j = np.arange(GROUP)
    forward = np.zeros((GROUP, n_r, width))
    back = np.zeros((n_r, piece.parts, piece.groups, width, piece.parts, piece.groups, GROUP))
    for row in range(n_r):
        for x in range(width):
            m = row * half + x % half
            cosine = x < half
            column = np.cos(2 * np.pi * j * m / GROUP) if cosine else np.sin(2 * np.pi * j * m / GROUP)
            entries = [(m, 1.0)]
            if not cosine and m == 0:
                column = np.cos(np.pi * j)
                entries = [(GROUP // 2, 1.0)]
            elif m:
                entries = [(m, 1.0 if cosine else -1.0), (GROUP - m, 1.0)]
            forward[:, row, x] = column
            for q in range(piece.parts):
                for g in range(piece.groups):
                    for at, sign in entries:
                        back[row, q, g, x, q, g, at] = sign
    size = piece.parts * piece.channels
    return forward.reshape(GROUP, LANES), back.reshape(n_r * LANES, size)


def position_tables(piece, rows_first, rows_second, n_r, n_c):
    length_first = rows_first * n_r
    length_second = rows_second * n_c
    positions = length_first * length_second
    block, parts, seconds = piece.block, piece.parts, piece.seconds
    half = block // 2
    a = np.arange(length_first)
    first = np.zeros((n_c, parts, n_c, piece.rows2, n_r, seconds, rows_first))
    for col in range(n_c):
        for i in range(rows_second):
            q, j = divmod(i, seconds)
            p = a * length_second + col * rows_second + i
            for target in range(n_c):
                for f_at in range(half):
                    f = target * half + f_at
                    angle = 2 * np.pi * (f * p % positions) / positions
                    real, imag = np.cos(angle), -np.sin(angle)
                    if f == 0:
                        real, imag = np.ones(length_first), (-1.0) ** a
                    first[col, q, target, j * block + 2 * f_at, :, j, :] = real.reshape(n_r, rows_first)
                    first[col, q, target, j * block + 2 * f_at + 1, :, j, :] = imag.reshape(n_r, rows_first)
    k_b = np.arange(length_second)
    plain = np.zeros((2, 2, length_second, block, parts, n_c, piece.rows2))
    for other in range(2):
        for s in range(block):
            for source in range(n_c):
                for i in range(rows_second):
                    b = source * rows_second + i
                    f_at, upper = s % half, s >= half
                    q, j = divmod(i, seconds)
                    re_at, im_at = (q, source, j * block + 2 * f_at), (q, source, j * block + 2 * f_at + 1)
                    if other == 0 and f_at == 0:
                        shift = length_first // 2 if upper else 0
                        angle = 2 * np.pi * (b * (k_b * length_first + shift) % positions) / positions
                        place = im_at if upper else re_at
                        plain[(other, 0, slice(None), s) + place] = np.cos(angle)
                        plain[(other, 1, slice(None), s) + place] = np.sin(angle)
                        continue
                    sign = -1.0 if upper else 1.0
                    angle = 2 * np.pi * (b * (k_b + (1 if upper else 0)) % length_second) / length_second
                    plain[(other, 0, slice(None), s) + re_at] = np.cos(angle)
                    plain[(other, 0, slice(None), s) + im_at] = np.sin(angle) * sign
                    plain[(other, 1, slice(None), s) + re_at] = np.sin(angle)
                    plain[(other, 1, slice(None), s) + im_at] = -np.cos(angle) * sign
    plain = plain.reshape(2, 2, n_r, piece.out_rows, parts, n_c * piece.rows2) / math.sqrt(positions * GROUP)
    second = np.zeros((2, n_r, parts, 2, piece.rows3, parts, n_c * piece.rows2))
    for q in range(parts):
        lo, hi = q * piece.rows3, min(piece.out_rows, (q + 1) * piece.rows3)
        for d in range(parts):
            values = plain[:, :, :, lo:hi, (q - d) % parts]
            second[:, :, q, :, : hi - lo, d] = values.transpose(0, 2, 1, 3, 4)
    first = first.reshape(n_c, parts * n_c * piece.rows2, n_r * piece.rows1)
    return first, second.reshape(2, n_r, parts * 2 * piece.rows3, parts * n_c * piece.rows2)


def bits_apart(one, other, count):
    total, bit = 0, 1
    while bit < count:
        total = total + bit * ((one // bit + other // bit) % 2)
        bit *= 2
    return total


def far_first(me, count):
    places = []
    for k in range(count - 1):
        down = count - 1 - k - jnp.where(count - 1 - k <= me, 1, 0)
        up = k + jnp.where(k >= me, 1, 0)
        places.append(jnp.where(me < count // 2, down, up))
    return places


def origin_first(me, count):
    places = far_first(me, count)
    inside = (me > 0) & (me < count // 2)
    return [jnp.where(inside, before, place) for before, place in zip([0] + places[:-1], places)]


def kernel(n_r, n_c, pieces, kinds, *refs):
    refs = list(refs)

    def take(count):
        taken = refs[:count]
        del refs[:count]
        return taken

    many = len(pieces)
    tokens, gain, w_in, w_out = take(4)
    (forward,) = take(1)
    tables_hbm = [take(3) for _ in pieces]
    partial, spectrum, tail_w = take(3)
    tok_v, gain_v, norm_v, win_v, early_v, wout_v, forward_v = take(7)
    tables_v = [take(3) for _ in pieces]
    buffers = [take(6) for _ in pieces]
    load_sem, out_sem, table_sem, send_sem, recv_sem = take(5)
    row, col = lax.axis_index("row"), lax.axis_index("col")
    rows, features = tokens.shape
    steps = len(kinds)
    spans, seats = [], []
    lo = 0
    for at, kind in enumerate(kinds):
        spans.append((lo, lo + pieces[kind].channels))
        seats.append(kinds[:at].count(kind))
        lo = spans[-1][1]

    barrier = pltpu.get_barrier_semaphore()
    for d in range(1, n_r):
        pl.semaphore_signal(barrier, inc=1, device_id={"row": bits_apart(row, d, n_r)}, device_id_type=MESH)
    for d in range(1, n_c):
        pl.semaphore_signal(barrier, inc=1, device_id={"col": bits_apart(col, d, n_c)}, device_id_type=MESH)

    load_tok = pltpu.make_async_copy(tokens, tok_v, load_sem.at[0])
    load_forward = pltpu.make_async_copy(forward, forward_v, load_sem.at[2])
    load_gain = pltpu.make_async_copy(gain, gain_v, load_sem.at[1])
    load_win = [
        pltpu.make_async_copy(w_in.at[:, lo:hi], win_v.at[:, lo:hi], load_sem.at[3 + t])
        for t, (lo, hi) in enumerate(spans)
    ]
    load = []
    for p, (first, second, back) in enumerate(tables_hbm):
        sources = (first.at[col], second.at[jnp.minimum(col, 1)], back)
        load.append(
            [pltpu.make_async_copy(x, y, table_sem.at[p, n]) for n, (x, y) in enumerate(zip(sources, tables_v[p]))]
        )
    head = spans[steps - TAIL][0]
    load_wout = [
        pltpu.make_async_copy(w_out.at[:head], wout_v, out_sem.at[0]),
        pltpu.make_async_copy(w_out.at[head:], tail_w, out_sem.at[1]),
    ]
    load_tok.start()
    load_gain.start()
    load_forward.start()
    load_win[0].start()
    pending = {(p, n) for p in range(many) for n in range(3)}

    def table(p, n):
        if (p, n) in pending:
            load[p][n].wait()
            pending.discard((p, n))
        return tables_v[p][n]

    load_tok.wait()
    load_gain.wait()
    gains = gain_v[...].astype(jnp.float32)
    squares = jnp.zeros((rows, LANES), jnp.float32)
    for at in range(features // LANES):
        lanes = slice(at * LANES, (at + 1) * LANES)
        floats = tok_v[:, lanes].astype(jnp.float32)
        squares = squares + floats * floats
        norm_v[:, lanes] = (floats * gains[at : at + 1, :]).astype(jnp.bfloat16)
    inverse = lax.rsqrt(jnp.sum(squares, axis=-1, keepdims=True) / features + norm_eps)

    row_targets = far_first(row, n_r)
    col_targets = [k + jnp.where(k >= col, 1, 0) for k in range(n_c - 1)]
    stages = ((row, row_targets, "row"), (col, col_targets, "col"), (row, origin_first(row, n_r), "row"))

    def exchange(stage, t, span=slice(None)):
        p, seat = kinds[t], seats[t]
        sent, came = buffers[p][2 * stage : 2 * stage + 2]
        me, targets, axis = stages[stage]
        for target in targets[span]:
            pltpu.make_async_remote_copy(
                src_ref=sent.at[seat, target],
                dst_ref=came.at[seat, me],
                send_sem=send_sem.at[stage, p],
                recv_sem=recv_sem.at[stage, t],
                device_id={axis: target},
                device_id_type=MESH,
            ).start()

    def keep(stage, t):
        p, seat = kinds[t], seats[t]
        sent, came = buffers[p][2 * stage : 2 * stage + 2]
        me = stages[stage][0]
        pltpu.make_async_copy(sent.at[seat, me], came.at[seat, me], recv_sem.at[stage, t]).start()

    def arrived(stage, t):
        came = buffers[kinds[t]][2 * stage + 1].at[seats[t]]
        pltpu.make_async_copy(came, came, recv_sem.at[stage, t]).wait()
        return came

    def all_sent():
        for stage, (_, targets, _) in enumerate(stages):
            for p in range(many):
                gone = buffers[p][2 * stage].at[:, 0 : len(targets)]
                pltpu.make_async_copy(gone, gone, send_sem.at[stage, p]).wait()

    lane = lax.broadcasted_iota(jnp.int32, (1, LANES), 1)
    turn = lane % (GROUP // n_r)
    cosine = (turn < GROUP // n_r // 2) | ((turn == GROUP // n_r // 2) & (row == 0))

    def start(t):
        p, seat = kinds[t], seats[t]
        piece = pieces[p]
        lo, hi = spans[t]
        load_win[t].wait()
        if t == 0:
            load_forward.wait()
            for other in load_win[1:]:
                other.start()
            for n in range(2):
                for other in sorted(range(many), key=kinds.index):
                    load[other][n].start()
        mapped = jnp.dot(norm_v[...], win_v[:, lo:hi], preferred_element_type=jnp.float32) * inverse
        short = piece.parts * piece.rows1 - rows
        if short:
            mapped = jnp.concatenate([mapped, jnp.zeros((short, hi - lo), jnp.float32)], axis=0)
        blocks = [
            mapped[q * piece.rows1 : (q + 1) * piece.rows1, g * GROUP : (g + 1) * GROUP]
            for q in range(piece.parts)
            for g in range(piece.groups)
        ]
        side = jnp.concatenate(blocks, axis=0).astype(jnp.bfloat16)
        turned = jnp.dot(side, forward_v[...], preferred_element_type=jnp.float32)
        sent = buffers[p][0]
        width = GROUP // n_r
        for r in range(n_r):
            total = None
            for k in range(len(blocks)):
                strip = turned[k * piece.rows1 : (k + 1) * piece.rows1]
                if k != r:
                    strip = pltpu.roll(strip, (k - r) * width % LANES, 1)
                total = strip if total is None else jnp.where(lane < k * width, total, strip)
            sent[seat, r] = total.astype(jnp.bfloat16)
        if t == 0:
            pl.semaphore_wait(barrier, n_r + n_c - 2)
        exchange(0, t)
        keep(0, t)

    def middle_first(t):
        p, seat = kinds[t], seats[t]
        piece = pieces[p]
        weights = table(p, 0)
        values = arrived(0, t)[...].reshape(n_r * piece.rows1, LANES)
        both = jnp.dot(weights[...], values, preferred_element_type=jnp.float32)
        size = n_c * piece.rows2
        total = both[:size]
        for q in range(1, piece.parts):
            total = jnp.where(lane < q * piece.used, total, both[q * size : (q + 1) * size])
        buffers[p][2][seat] = total.astype(jnp.bfloat16).reshape(n_c, piece.rows2, LANES)
        exchange(1, t)
        keep(1, t)

    def middle_second(t):
        p, seat = kinds[t], seats[t]
        piece = pieces[p]
        weights = table(p, 1)
        values = arrived(1, t)[...].reshape(n_c * piece.rows2, LANES)
        floats = values.astype(jnp.float32)
        rolled = [values] + [
            pltpu.roll(floats, d * piece.used, 1).astype(jnp.bfloat16) for d in range(1, piece.parts)
        ]
        deep = jnp.concatenate(rolled, axis=0)
        sent = buffers[p][4]
        size = piece.rows3
        for r in range(n_r):
            both = jnp.dot(weights[r], deep, preferred_element_type=jnp.float32)
            chosen = [
                jnp.where(cosine, both[2 * q * size : (2 * q + 1) * size], both[(2 * q + 1) * size : (2 * q + 2) * size])
                for q in range(piece.parts)
            ]
            total = chosen[0]
            for q in range(1, piece.parts):
                total = jnp.where(lane < q * piece.used, total, chosen[q])
            sent[seat, r] = total.astype(jnp.bfloat16)
        exchange(2, t, slice(0, 1))
        if t < steps - HELD:
            exchange(2, t, slice(1, None))
        else:

            @pl.when(row < n_r // 2)
            def _():
                exchange(2, t, slice(1, None))

        if t == steps - 1:

            @pl.when(row >= n_r // 2)
            def _():
                for held in range(steps - HELD, steps):
                    exchange(2, held, slice(1, None))

        keep(2, t)

    def finish(t):
        p, seat = kinds[t], seats[t]
        piece = pieces[p]
        lo, hi = spans[t]
        weights = table(p, 2)
        came = arrived(2, t)
        side = jnp.concatenate([came[r] for r in range(n_r)], axis=1)
        total = jnp.dot(side, weights[...], preferred_element_type=jnp.float32).astype(jnp.bfloat16)
        size = piece.channels
        place, lo = (early_v, lo) if t < steps - TAIL else (spectrum, lo - head)
        for q in range(piece.parts):
            above, below = q * piece.rows3, min(piece.out_rows, (q + 1) * piece.rows3)
            place[above:below, lo : lo + size] = total[: below - above, q * size : (q + 1) * size]
        if t == steps - TAIL - 1:
            load_wout[0].wait()
            for at in range(0, features, COLUMNS):
                columns = slice(at, at + COLUMNS)
                partial[:, columns] = jnp.dot(early_v[...], wout_v[:, columns], preferred_element_type=jnp.float32)
            load_wout[1].wait()

    for t in range(steps):
        start(t)
    for p in range(many):
        load[p][2].start()
    for copy in load_wout:
        copy.start()
    for job, t in schedule(steps):
        (middle_first, middle_second, finish)[job](t)
    all_sent()


def schedule(steps):
    jobs = [(0, t) for t in range(steps)]
    jobs[min(LAG, steps) : min(LAG, steps)] = [(1, 0)]
    return jobs + [(1, t) for t in range(1, steps)] + [(2, t) for t in range(steps)]


def last_product(partial, spectrum, w_tail, out, out_v, sems):
    copies = []
    for n, at in enumerate(range(0, partial.shape[1], COLUMNS)):
        columns = slice(at, at + COLUMNS)
        total = jnp.dot(spectrum[...], w_tail[:, columns], preferred_element_type=jnp.float32)
        total = total + partial[:, columns]
        out_v[:, :, columns] = total.reshape(*out_v.shape[:2], COLUMNS).astype(jnp.bfloat16)
        copy = pltpu.make_async_copy(out_v.at[:, :, columns], out.at[:, :, columns], sems.at[n])
        copy.start()
        copies.append(copy)
    for copy in copies:
        copy.wait()


def fused_shards(n_r, n_c, tokens, norm_gain, w_in, w_out):
    rows_first, rows_second, features = tokens.shape
    channels = w_in.shape[1]
    length_second = rows_second * n_c
    sizes = chunk_sizes(channels // GROUP, n_r)
    distinct = sorted(set(sizes))
    kinds = [distinct.index(size) for size in sizes]
    pieces = [Piece(size, n_r, n_c, rows_first, rows_second, length_second) for size in distinct]
    block, out_rows = pieces[0].block, pieces[0].out_rows
    head = sum(sizes[:-TAIL]) * GROUP
    rows = rows_first * rows_second
    tokens = tokens.transpose(1, 0, 2).reshape(rows, features)
    kind = jnp.bfloat16
    tables = [channel_tables(pieces[0], n_r)[0]]
    for piece in pieces:
        _, back = channel_tables(piece, n_r)
        first, second = position_tables(piece, rows_first, rows_second, n_r, n_c)
        tables += [first, second, back]
    tables = [jnp.asarray(np.asarray(x, np.float32).astype(kind)) for x in tables]
    hbm = pl.BlockSpec(memory_space=pltpu.HBM)
    vmem = pl.BlockSpec(memory_space=pltpu.VMEM)
    dma = pltpu.SemaphoreType.DMA
    scratch = [
        pltpu.VMEM((rows, features), kind),
        pltpu.VMEM((features // LANES, LANES), kind),
        pltpu.VMEM((rows, features), kind),
        pltpu.VMEM(w_in.shape, kind),
        pltpu.VMEM((out_rows, head), kind),
        pltpu.VMEM((head, features), kind),
        pltpu.VMEM(tables[0].shape, kind),
    ]
    for p in range(len(pieces)):
        first, second, back = tables[3 * p + 1 : 3 * p + 4]
        scratch += [pltpu.VMEM(x, kind) for x in (first.shape[1:], second.shape[1:], back.shape)]
    for p, piece in enumerate(pieces):
        count = kinds.count(p)
        for first_size, second_size in ((n_r, piece.rows1), (n_c, piece.rows2), (n_r, piece.rows3)):
            scratch += [pltpu.VMEM((count, first_size, second_size, LANES), kind)] * 2
    steps = len(kinds)
    scratch += [dma((3 + steps,)), dma((2,)), dma((len(pieces), 3)), dma((3, len(pieces))), dma((3, steps))]
    operands = (tokens, norm_gain.reshape(-1, LANES), w_in, w_out, *tables)
    partial, spectrum, w_tail = pl.pallas_call(
        functools.partial(kernel, n_r, n_c, pieces, kinds),
        out_shape=[
            pltpu.VMEM((out_rows, features), jnp.float32),
            pltpu.VMEM((out_rows, channels - head), kind),
            pltpu.VMEM((channels - head, features), kind),
        ],
        in_specs=[hbm] * len(operands),
        out_specs=[vmem] * 3,
        scratch_shapes=scratch,
        compiler_params=pltpu.CompilerParams(
            collective_id=0, has_side_effects=True, vmem_limit_bytes=53 * 1024 * 1024
        ),
    )(*[pltpu.with_memory_space_constraint(x, pltpu.HBM) for x in operands])
    out_shape = (length_second // n_r, block, features)
    return pl.pallas_call(
        last_product,
        out_shape=jax.ShapeDtypeStruct(out_shape, kind),
        in_specs=[vmem] * 3,
        out_specs=hbm,
        scratch_shapes=[pltpu.VMEM(out_shape, kind), dma((features // COLUMNS,))],
        compiler_params=pltpu.CompilerParams(vmem_limit_bytes=16 * 1024 * 1024),
    )(partial, spectrum, w_tail)


def fits(n_r, n_c, tokens_shape, channels):
    length_first, length_second, features = tokens_shape
    return (
        n_r > 1
        and n_c & (n_c - 1) == 0
        and GROUP % (2 * n_r) == 0
        and length_first % (2 * n_c) == 0
        and SUBLANES % (length_first // n_c) == 0
        and length_first // n_r % ROWS == 0
        and length_second // n_r * (length_first // n_c) % ROWS == 0
        and length_second % n_r == 0
        and features % COLUMNS == 0
        and len(chunk_sizes(channels // GROUP, n_r)) > TAIL
        and all(LANES % (size * GROUP // n_r) == 0 for size in chunk_sizes(channels // GROUP, n_r))
    )


def tables(length):
    series = jnp.arange(length, dtype=jnp.int32)
    product = series[:, None] * series[None, :] % length
    angles = product.astype(jnp.float32) * (2.0 * math.pi / length)
    return (jnp.cos(angles), jnp.sin(angles))


def folded_order(length_first, devices):
    block = length_first // devices
    half_block = block // 2
    series = jnp.arange(length_first, dtype=jnp.int32)
    device = series // block
    inner = series % block
    lower = device * half_block + inner
    upper = length_first - device * half_block - (inner - half_block)
    upper = jnp.where((device == 0) & (inner == half_block), length_first // 2, upper)
    return jnp.where(inner < half_block, lower, upper) % length_first


def to_channels(values, row_count):
    rows_first, rows_second, channels = values.shape
    width = channels // row_count
    parted = values.reshape(rows_first, rows_second, row_count, width).transpose(2, 0, 1, 3)
    return parted.reshape(row_count * rows_first, rows_second * width)


def product(table, values):
    return jnp.dot(table, values, precision=highest)


def middle(real_part, imag_part, width):
    length_first = real_part.shape[0]
    rows_second = real_part.shape[1] // width
    col_count = lax.axis_size("col")
    length_second = rows_second * col_count
    positions = length_first * length_second
    frequency = folded_order(length_first, col_count)
    series = jnp.arange(length_first, dtype=jnp.int32)
    first_angle = (frequency[:, None] * series[None, :] % length_first).astype(jnp.float32)
    first_angle = first_angle * (2.0 * math.pi / length_first)
    first_cos = jnp.cos(first_angle)
    first_sin = jnp.sin(first_angle)
    first_real = product(first_cos, real_part)
    first_imag = -product(first_sin, real_part)
    first_real = first_real + product(first_sin, imag_part)
    first_imag = first_imag + product(first_cos, imag_part)
    first_real = first_real.reshape(length_first, rows_second, width)
    first_imag = first_imag.reshape(length_first, rows_second, width)
    second_index = lax.axis_index("col") * rows_second + jnp.arange(rows_second, dtype=jnp.int32)
    twiddle_angle = (frequency[:, None] * second_index[None, :] % positions).astype(jnp.float32)
    twiddle_angle = twiddle_angle * (2.0 * math.pi / positions)
    twiddle_cos = jnp.cos(twiddle_angle)[:, :, None]
    twiddle_sin = jnp.sin(twiddle_angle)[:, :, None]
    turned_real = first_real * twiddle_cos + first_imag * twiddle_sin
    turned_imag = first_imag * twiddle_cos - first_real * twiddle_sin
    turned = jnp.stack([turned_real, turned_imag]).transpose(0, 2, 1, 3)
    turned = turned.reshape(2, rows_second, length_first * width)
    exchanged = lax.all_to_all(
        turned.astype(jnp.bfloat16), "col", split_axis=2, concat_axis=1, tiled=True
    ).astype(turned.dtype)
    second_cos, second_sin = tables(length_second)
    block = length_first // col_count
    out_shape = (length_second, block, width)
    out_real = (product(second_cos, exchanged[0]) + product(second_sin, exchanged[1])).reshape(
        out_shape
    )
    return out_real


def shards(tokens, norm_gain, w_in, w_out):
    rows_first, rows_second, features = tokens.shape
    row_count = lax.axis_size("row")
    length_first = rows_first * row_count
    length_second = rows_second * lax.axis_size("col")
    channels = w_in.shape[1]
    width = channels // row_count
    groups = channels // GROUP
    scaling = 1.0 / math.sqrt(length_first * length_second * GROUP)
    floats = tokens.astype(jnp.float32)
    normed = (
        floats
        * lax.rsqrt(jnp.mean(floats * floats, axis=-1, keepdims=True) + norm_eps)
        * norm_gain.astype(jnp.float32)
    ).astype(jnp.bfloat16)
    mapped = jnp.dot(normed.reshape(-1, features), w_in, preferred_element_type=jnp.float32)
    mapped = mapped.astype(jnp.bfloat16).reshape(rows_first, rows_second, channels)
    channel_cos, channel_sin = tables(GROUP)
    grouped = mapped.astype(jnp.float32).reshape(rows_first, rows_second, groups, GROUP)
    spec_real = jnp.einsum("abgj,jm->abgm", grouped, channel_cos, precision=highest)
    spec_imag = -jnp.einsum("abgj,jm->abgm", grouped, channel_sin, precision=highest)
    stacked = jnp.stack(
        [
            to_channels(spec_real.reshape(rows_first, rows_second, channels), row_count),
            to_channels(spec_imag.reshape(rows_first, rows_second, channels), row_count),
        ]
    )
    arrived = lax.all_to_all(
        stacked.astype(jnp.bfloat16), "row", split_axis=1, concat_axis=1, tiled=True
    ).astype(stacked.dtype)
    result = middle(arrived[0], arrived[1], width)
    spectrum = (result * scaling).astype(jnp.bfloat16)
    returned = lax.all_to_all(spectrum, "row", split_axis=0, concat_axis=2, tiled=True)
    mixed = jnp.dot(returned.reshape(-1, channels), w_out, preferred_element_type=jnp.float32)
    return mixed.astype(jnp.bfloat16).reshape(returned.shape[0], returned.shape[1], features)


def solution(mesh):
    in_specs = (P("row", "col", None), P(), P(), P())
    out_specs = P("row", "col", None)
    n_r, n_c = mesh.shape["row"], mesh.shape["col"]

    def run(tokens, norm_gain, w_in, w_out):
        whole = fits(n_r, n_c, tokens.shape, w_in.shape[1])
        body = functools.partial(fused_shards, n_r, n_c) if whole else shards
        return jax.shard_map(body, mesh=mesh, in_specs=in_specs, out_specs=out_specs, check_vma=False)(
            tokens, norm_gain, w_in, w_out
        )

    return run
```

```python
import functools
import math

import jax
import jax.numpy as jnp
import numpy as np
from jax import lax
from jax.experimental import pallas as pl
from jax.experimental.pallas import tpu as pltpu
from jax.sharding import PartitionSpec as P

GROUP = 128
LANES = 128
SUBLANES = 16
ROWS = 8
LAG = 3
TAIL = 2
HELD = 3
COLUMNS = 512
MESH = pl.DeviceIdType.MESH


norm_eps = 1e-06
highest = lax.Precision.HIGHEST


def folded_list(length_first, devices):
    block = length_first // devices
    half = block // 2
    result = np.zeros(length_first, np.int64)
    for device in range(devices):
        for inner in range(block):
            if inner < half:
                value = device * half + inner
            elif device == 0 and inner == half:
                value = length_first // 2
            else:
                value = length_first - device * half - (inner - half)
            result[device * block + inner] = value % length_first
    return result


def ceil_to(value, multiple):
    return -(-value // multiple) * multiple


class Piece:
    def __init__(self, groups, n_r, n_c, rows_first, rows_second, length_second):
        self.groups = groups
        self.channels = groups * GROUP
        self.used = groups * GROUP // n_r
        self.parts = LANES // self.used
        self.seconds = -(-rows_second // self.parts)
        self.block = rows_first * n_r // n_c
        self.rows1 = self.seconds * rows_first
        self.rows2 = ceil_to(self.seconds * self.block, ROWS)
        self.out_rows = length_second // n_r * self.block
        self.half = self.block // 2
        self.strips = self.parts // self.half
        self.step = self.out_rows // self.half // max(1, self.strips)
        self.rows3 = ceil_to(self.step, ROWS)
        depth = 2 * self.seconds
        ends = [(f * depth // ROWS * ROWS, ceil_to((f + 1) * depth, ROWS)) for f in range(self.half)]
        self.window = max(hi - lo for lo, hi in ends)
        self.lows = [min(lo, self.rows2 - self.window) for lo, _ in ends]


def chunk_sizes(groups, n_r):
    per = LANES // 2 // (GROUP // n_r)
    rest = groups % per
    return [per] * (groups // per) + ([rest] if rest else [])


def channel_tables(piece, n_r):
    width = GROUP // n_r
    half = width // 2
    j = np.arange(GROUP)
    forward = np.zeros((GROUP, n_r, width))
    back = np.zeros((n_r, piece.parts, piece.groups, width, piece.parts, piece.groups, GROUP))
    for row in range(n_r):
        for x in range(width):
            m = row * half + x % half
            cosine = x < half
            column = np.cos(2 * np.pi * j * m / GROUP) if cosine else np.sin(2 * np.pi * j * m / GROUP)
            entries = [(m, 1.0)]
            if not cosine and m == 0:
                column = np.cos(np.pi * j)
                entries = [(GROUP // 2, 1.0)]
            elif m:
                entries = [(m, 1.0 if cosine else -1.0), (GROUP - m, 1.0)]
            forward[:, row, x] = column
            for q in range(piece.parts):
                for g in range(piece.groups):
                    for at, sign in entries:
                        back[row, q, g, x, q, g, at] = sign
    size = piece.parts * piece.channels
    return forward.reshape(GROUP, LANES), back.reshape(n_r * LANES, size)


def position_tables(piece, rows_first, rows_second, n_r, n_c):
    length_first = rows_first * n_r
    length_second = rows_second * n_c
    positions = length_first * length_second
    block, parts, seconds = piece.block, piece.parts, piece.seconds
    half = block // 2
    a = np.arange(length_first)
    first = np.zeros((n_c, n_c, piece.rows2, n_r, seconds, rows_first))
    for col in range(n_c):
        for j in range(seconds):
            p = a * length_second + col * rows_second + j
            for target in range(n_c):
                for f_at in range(half):
                    f = target * half + f_at
                    angle = 2 * np.pi * (f * p % positions) / positions
                    real, imag = np.cos(angle), -np.sin(angle)
                    if f == 0:
                        real, imag = np.ones(length_first), (-1.0) ** a
                    first[col, target, 2 * (f_at * seconds + j), :, j, :] = real.reshape(n_r, rows_first)
                    first[col, target, 2 * (f_at * seconds + j) + 1, :, j, :] = imag.reshape(n_r, rows_first)
    k_b = np.arange(length_second)
    plain = np.zeros((2, 2, length_second, block, parts, n_c, piece.rows2))
    for other in range(2):
        for s in range(block):
            for source in range(n_c):
                for i in range(rows_second):
                    b = source * rows_second + i
                    f_at, upper = s % half, s >= half
                    q, j = divmod(i, seconds)
                    at = 2 * (f_at * seconds + j)
                    re_at, im_at = (q, source, at), (q, source, at + 1)
                    if other == 0 and f_at == 0:
                        shift = length_first // 2 if upper else 0
                        angle = 2 * np.pi * (b * (k_b * length_first + shift) % positions) / positions
                        place = im_at if upper else re_at
                        plain[(other, 0, slice(None), s) + place] = np.cos(angle)
                        plain[(other, 1, slice(None), s) + place] = np.sin(angle)
                        continue
                    sign = -1.0 if upper else 1.0
                    angle = 2 * np.pi * (b * (k_b + (1 if upper else 0)) % length_second) / length_second
                    plain[(other, 0, slice(None), s) + re_at] = np.cos(angle)
                    plain[(other, 0, slice(None), s) + im_at] = np.sin(angle) * sign
                    plain[(other, 1, slice(None), s) + re_at] = np.sin(angle)
                    plain[(other, 1, slice(None), s) + im_at] = -np.cos(angle) * sign
    plain = plain.reshape(2, 2, n_r, piece.out_rows, parts, n_c, piece.rows2) / math.sqrt(positions * GROUP)
    strips, step, window = piece.strips, piece.step, piece.window
    second = np.zeros((n_c, half, n_r, strips, 2, piece.rows3, parts, n_c, window))
    for col in range(n_c):
        mine = plain[min(col, 1)].copy()
        for f_at in range(half):
            f = col * half + f_at
            for q in range(parts if f else 0):
                turn = 2 * np.pi * (f * q * seconds % positions) / positions
                lo, hi = 2 * f_at * seconds, 2 * (f_at + 1) * seconds
                real, imag = mine[..., q, :, lo:hi:2].copy(), mine[..., q, :, lo + 1 : hi : 2].copy()
                mine[..., q, :, lo:hi:2] = real * np.cos(turn) - imag * np.sin(turn)
                mine[..., q, :, lo + 1 : hi : 2] = real * np.sin(turn) + imag * np.cos(turn)
        for f in range(half):
            low = piece.lows[f]
            for h in range(strips):
                rows = half * (h * step + np.arange(step)) + f
                for d in range(parts):
                    values = mine[:, :, rows, (f * strips + h - d) % parts, :, low : low + window]
                    second[col, f, :, h, :, :step, d] = values.transpose(1, 0, 2, 3, 4)
    first = first.reshape(n_c, n_c * piece.rows2, n_r * piece.rows1)
    return first, second.reshape(n_c, half, n_r * strips * 2 * piece.rows3, parts * n_c * window)


def bits_apart(one, other, count):
    total, bit = 0, 1
    while bit < count:
        total = total + bit * ((one // bit + other // bit) % 2)
        bit *= 2
    return total


def far_first(me, count):
    places = []
    for k in range(count - 1):
        down = count - 1 - k - jnp.where(count - 1 - k <= me, 1, 0)
        up = k + jnp.where(k >= me, 1, 0)
        places.append(jnp.where(me < count // 2, down, up))
    return places


def origin_first(me, count):
    places = far_first(me, count)
    inside = (me > 0) & (me < count // 2)
    return [jnp.where(inside, before, place) for before, place in zip([0] + places[:-1], places)]


def kernel(n_r, n_c, pieces, kinds, *refs):
    refs = list(refs)

    def take(count):
        taken = refs[:count]
        del refs[:count]
        return taken

    many = len(pieces)
    tokens, gain, w_in, w_out = take(4)
    (forward,) = take(1)
    tables_hbm = [take(3) for _ in pieces]
    partial, spectrum, tail_w = take(3)
    tok_v, gain_v, norm_v, win_v, early_v, wout_v, forward_v, woven_v = take(8)
    tables_v = [take(3) for _ in pieces]
    buffers = [take(6) for _ in pieces]
    load_sem, out_sem, table_sem, send_sem, recv_sem = take(5)
    row, col = lax.axis_index("row"), lax.axis_index("col")
    rows, features = tokens.shape
    steps = len(kinds)
    spans, seats = [], []
    lo = 0
    for at, kind in enumerate(kinds):
        spans.append((lo, lo + pieces[kind].channels))
        seats.append(kinds[:at].count(kind))
        lo = spans[-1][1]

    barrier = pltpu.get_barrier_semaphore()
    for d in range(1, n_r):
        pl.semaphore_signal(barrier, inc=1, device_id={"row": bits_apart(row, d, n_r)}, device_id_type=MESH)
    for d in range(1, n_c):
        pl.semaphore_signal(barrier, inc=1, device_id={"col": bits_apart(col, d, n_c)}, device_id_type=MESH)

    load_tok = pltpu.make_async_copy(tokens, tok_v, load_sem.at[0])
    load_forward = pltpu.make_async_copy(forward, forward_v, load_sem.at[2])
    load_gain = pltpu.make_async_copy(gain, gain_v, load_sem.at[1])
    load_win = [
        pltpu.make_async_copy(w_in.at[:, lo:hi], win_v.at[:, lo:hi], load_sem.at[3 + t])
        for t, (lo, hi) in enumerate(spans)
    ]
    load = []
    for p, (first, second, back) in enumerate(tables_hbm):
        sources = (first.at[col], second.at[col], back)
        load.append(
            [pltpu.make_async_copy(x, y, table_sem.at[p, n]) for n, (x, y) in enumerate(zip(sources, tables_v[p]))]
        )
    head = spans[steps - TAIL][0]
    load_wout = [
        pltpu.make_async_copy(w_out.at[:head], wout_v, out_sem.at[0]),
        pltpu.make_async_copy(w_out.at[head:], tail_w, out_sem.at[1]),
    ]
    load_tok.start()
    load_gain.start()
    load_forward.start()
    load_win[0].start()
    pending = {(p, n) for p in range(many) for n in range(3)}

    def table(p, n):
        if (p, n) in pending:
            load[p][n].wait()
            pending.discard((p, n))
        return tables_v[p][n]

    load_tok.wait()
    load_gain.wait()
    gains = gain_v[...].astype(jnp.float32)
    squares = jnp.zeros((rows, LANES), jnp.float32)
    for at in range(features // LANES):
        lanes = slice(at * LANES, (at + 1) * LANES)
        floats = tok_v[:, lanes].astype(jnp.float32)
        squares = squares + floats * floats
        norm_v[:, lanes] = (floats * gains[at : at + 1, :]).astype(jnp.bfloat16)
    inverse = lax.rsqrt(jnp.sum(squares, axis=-1, keepdims=True) / features + norm_eps)

    row_targets = far_first(row, n_r)
    col_targets = [k + jnp.where(k >= col, 1, 0) for k in range(n_c - 1)]
    stages = ((row, row_targets, "row"), (col, col_targets, "col"), (row, origin_first(row, n_r), "row"))

    def exchange(stage, t, span=slice(None)):
        p, seat = kinds[t], seats[t]
        sent, came = buffers[p][2 * stage : 2 * stage + 2]
        me, targets, axis = stages[stage]
        for target in targets[span]:
            pltpu.make_async_remote_copy(
                src_ref=sent.at[seat, target],
                dst_ref=came.at[seat, me],
                send_sem=send_sem.at[stage, p],
                recv_sem=recv_sem.at[stage, t],
                device_id={axis: target},
                device_id_type=MESH,
            ).start()

    def keep(stage, t):
        p, seat = kinds[t], seats[t]
        sent, came = buffers[p][2 * stage : 2 * stage + 2]
        me = stages[stage][0]
        pltpu.make_async_copy(sent.at[seat, me], came.at[seat, me], recv_sem.at[stage, t]).start()

    def arrived(stage, t):
        came = buffers[kinds[t]][2 * stage + 1].at[seats[t]]
        pltpu.make_async_copy(came, came, recv_sem.at[stage, t]).wait()
        return came

    def all_sent():
        for stage, (_, targets, _) in enumerate(stages):
            for p in range(many):
                gone = buffers[p][2 * stage].at[:, 0 : len(targets)]
                pltpu.make_async_copy(gone, gone, send_sem.at[stage, p]).wait()

    lane = lax.broadcasted_iota(jnp.int32, (1, LANES), 1)
    turn = lane % (GROUP // n_r)
    cosine = (turn < GROUP // n_r // 2) | ((turn == GROUP // n_r // 2) & (row == 0))

    def start(t):
        p, seat = kinds[t], seats[t]
        piece = pieces[p]
        lo, hi = spans[t]
        load_win[t].wait()
        if t == 0:
            load_forward.wait()
            for other in load_win[1:]:
                other.start()
            for n in range(2):
                for other in sorted(range(many), key=kinds.index):
                    load[other][n].start()
        mapped = jnp.dot(norm_v[...], win_v[:, lo:hi], preferred_element_type=jnp.float32) * inverse
        short = piece.parts * piece.rows1 - rows
        if short:
            mapped = jnp.concatenate([mapped, jnp.zeros((short, hi - lo), jnp.float32)], axis=0)
        blocks = [
            mapped[q * piece.rows1 : (q + 1) * piece.rows1, g * GROUP : (g + 1) * GROUP]
            for q in range(piece.parts)
            for g in range(piece.groups)
        ]
        side = jnp.concatenate(blocks, axis=0).astype(jnp.bfloat16)
        turned = jnp.dot(side, forward_v[...], preferred_element_type=jnp.float32)
        sent = buffers[p][0]
        width = GROUP // n_r
        for r in range(n_r):
            total = None
            for k in range(len(blocks)):
                strip = turned[k * piece.rows1 : (k + 1) * piece.rows1]
                if k != r:
                    strip = pltpu.roll(strip, (k - r) * width % LANES, 1)
                total = strip if total is None else jnp.where(lane < k * width, total, strip)
            sent[seat, r] = total.astype(jnp.bfloat16)
        if t == 0:
            pl.semaphore_wait(barrier, n_r + n_c - 2)
        exchange(0, t)
        keep(0, t)

    def middle_first(t):
        p, seat = kinds[t], seats[t]
        piece = pieces[p]
        weights = table(p, 0)
        values = arrived(0, t)[...].reshape(n_r * piece.rows1, LANES)
        total = jnp.dot(weights[...], values, preferred_element_type=jnp.float32)
        buffers[p][2][seat] = total.astype(jnp.bfloat16).reshape(n_c, piece.rows2, LANES)
        exchange(1, t)
        keep(1, t)

    def middle_second(t):
        p, seat = kinds[t], seats[t]
        piece = pieces[p]
        weights = table(p, 1)
        values = arrived(1, t)
        sent = buffers[p][4]
        size = piece.rows3
        count = n_c * piece.window
        chosen = []
        for f, low in enumerate(piece.lows):
            floats = values[:, low : low + piece.window].reshape(count, LANES).astype(jnp.float32)
            rolled = [floats] + [pltpu.roll(floats, d * piece.used, 1) for d in range(1, piece.parts)]
            deep = jnp.concatenate([part.astype(jnp.bfloat16) for part in rolled], axis=0)
            both = jnp.dot(weights[f], deep, preferred_element_type=jnp.float32)
            blocks = [both[n * size : (n + 1) * size] for n in range(2 * n_r * piece.strips)]
            chosen.append([jnp.where(cosine, *blocks[n : n + 2]) for n in range(0, len(blocks), 2)])
        for r in range(n_r):
            total = None
            for q in range(piece.parts):
                f, h = divmod(q, piece.strips)
                part = chosen[f][r * piece.strips + h]
                total = part if total is None else jnp.where(lane < q * piece.used, total, part)
            sent[seat, r] = total.astype(jnp.bfloat16)
        exchange(2, t, slice(0, 1))
        if t < steps - HELD:
            exchange(2, t, slice(1, None))
        else:

            @pl.when(row < n_r // 2)
            def _():
                exchange(2, t, slice(1, None))

        if t == steps - 1:

            @pl.when(row >= n_r // 2)
            def _():
                for held in range(steps - HELD, steps):
                    exchange(2, held, slice(1, None))

        keep(2, t)

    def finish(t):
        p, seat = kinds[t], seats[t]
        piece = pieces[p]
        lo, hi = spans[t]
        weights = table(p, 2)
        came = arrived(2, t)
        side = jnp.concatenate([came[r] for r in range(n_r)], axis=1)
        total = jnp.dot(side, weights[...], preferred_element_type=jnp.float32)
        size, step = piece.channels, piece.step
        place, lo = (early_v, lo) if t < steps - TAIL else (spectrum, lo - head)
        for q in range(piece.parts):
            f, h = divmod(q, piece.strips)
            for c in range(size // LANES):
                at = q * size + c * LANES
                woven_v[c, pl.ds(piece.half * h * step + f, step, stride=piece.half), :] = total[:step, at : at + LANES]
        for c in range(size // LANES):
            place[:, lo + c * LANES : lo + (c + 1) * LANES] = woven_v[c].astype(jnp.bfloat16)
        if t == steps - TAIL - 1:
            load_wout[0].wait()
            for at in range(0, features, COLUMNS):
                columns = slice(at, at + COLUMNS)
                partial[:, columns] = jnp.dot(early_v[...], wout_v[:, columns], preferred_element_type=jnp.float32)
            load_wout[1].wait()

    for t in range(steps):
        start(t)
    for p in range(many):
        load[p][2].start()
    for copy in load_wout:
        copy.start()
    for job, t in schedule(steps):
        (middle_first, middle_second, finish)[job](t)
    all_sent()


def schedule(steps):
    jobs = [(0, t) for t in range(steps)]
    jobs[min(LAG, steps) : min(LAG, steps)] = [(1, 0)]
    return jobs + [(1, t) for t in range(1, steps)] + [(2, t) for t in range(steps)]


def last_product(partial, spectrum, w_tail, out, out_v, sems):
    copies = []
    for n, at in enumerate(range(0, partial.shape[1], COLUMNS)):
        columns = slice(at, at + COLUMNS)
        total = jnp.dot(spectrum[...], w_tail[:, columns], preferred_element_type=jnp.float32)
        total = total + partial[:, columns]
        out_v[:, :, columns] = total.reshape(*out_v.shape[:2], COLUMNS).astype(jnp.bfloat16)
        copy = pltpu.make_async_copy(out_v.at[:, :, columns], out.at[:, :, columns], sems.at[n])
        copy.start()
        copies.append(copy)
    for copy in copies:
        copy.wait()


def fused_shards(n_r, n_c, tokens, norm_gain, w_in, w_out):
    rows_first, rows_second, features = tokens.shape
    channels = w_in.shape[1]
    length_second = rows_second * n_c
    sizes = chunk_sizes(channels // GROUP, n_r)
    distinct = sorted(set(sizes))
    kinds = [distinct.index(size) for size in sizes]
    pieces = [Piece(size, n_r, n_c, rows_first, rows_second, length_second) for size in distinct]
    block, out_rows = pieces[0].block, pieces[0].out_rows
    head = sum(sizes[:-TAIL]) * GROUP
    rows = rows_first * rows_second
    tokens = tokens.transpose(1, 0, 2).reshape(rows, features)
    kind = jnp.bfloat16
    tables = [channel_tables(pieces[0], n_r)[0]]
    for piece in pieces:
        _, back = channel_tables(piece, n_r)
        first, second = position_tables(piece, rows_first, rows_second, n_r, n_c)
        tables += [first, second, back]
    tables = [jnp.asarray(np.asarray(x, np.float32).astype(kind)) for x in tables]
    hbm = pl.BlockSpec(memory_space=pltpu.HBM)
    vmem = pl.BlockSpec(memory_space=pltpu.VMEM)
    dma = pltpu.SemaphoreType.DMA
    scratch = [
        pltpu.VMEM((rows, features), kind),
        pltpu.VMEM((features // LANES, LANES), kind),
        pltpu.VMEM((rows, features), kind),
        pltpu.VMEM(w_in.shape, kind),
        pltpu.VMEM((out_rows, head), kind),
        pltpu.VMEM((head, features), kind),
        pltpu.VMEM(tables[0].shape, kind),
        pltpu.VMEM((max(sizes) * GROUP // LANES, out_rows, LANES), jnp.float32),
    ]
    for p in range(len(pieces)):
        first, second, back = tables[3 * p + 1 : 3 * p + 4]
        scratch += [pltpu.VMEM(x, kind) for x in (first.shape[1:], second.shape[1:], back.shape)]
    for p, piece in enumerate(pieces):
        count = kinds.count(p)
        for first_size, second_size in ((n_r, piece.rows1), (n_c, piece.rows2), (n_r, piece.rows3)):
            scratch += [pltpu.VMEM((count, first_size, second_size, LANES), kind)] * 2
    steps = len(kinds)
    scratch += [dma((3 + steps,)), dma((2,)), dma((len(pieces), 3)), dma((3, len(pieces))), dma((3, steps))]
    operands = (tokens, norm_gain.reshape(-1, LANES), w_in, w_out, *tables)
    partial, spectrum, w_tail = pl.pallas_call(
        functools.partial(kernel, n_r, n_c, pieces, kinds),
        out_shape=[
            pltpu.VMEM((out_rows, features), jnp.float32),
            pltpu.VMEM((out_rows, channels - head), kind),
            pltpu.VMEM((channels - head, features), kind),
        ],
        in_specs=[hbm] * len(operands),
        out_specs=[vmem] * 3,
        scratch_shapes=scratch,
        compiler_params=pltpu.CompilerParams(
            collective_id=0, has_side_effects=True, vmem_limit_bytes=53 * 1024 * 1024
        ),
    )(*[pltpu.with_memory_space_constraint(x, pltpu.HBM) for x in operands])
    out_shape = (length_second // n_r, block, features)
    return pl.pallas_call(
        last_product,
        out_shape=jax.ShapeDtypeStruct(out_shape, kind),
        in_specs=[vmem] * 3,
        out_specs=hbm,
        scratch_shapes=[pltpu.VMEM(out_shape, kind), dma((features // COLUMNS,))],
        compiler_params=pltpu.CompilerParams(vmem_limit_bytes=16 * 1024 * 1024),
    )(partial, spectrum, w_tail)


def divided(n_r, n_c, length_first, length_second, size):
    used, half = size * GROUP // n_r, length_first // n_c // 2
    out_rows = length_second // n_r * 2 * half
    return LANES % (used * half) == 0 and out_rows % (LANES // used) == 0


def fits(n_r, n_c, tokens_shape, channels):
    length_first, length_second, features = tokens_shape
    return (
        n_r > 1
        and n_c & (n_c - 1) == 0
        and GROUP % (2 * n_r) == 0
        and length_first % (2 * n_c) == 0
        and SUBLANES % (length_first // n_c) == 0
        and length_first // n_r % ROWS == 0
        and length_second // n_r * (length_first // n_c) % ROWS == 0
        and length_second % n_r == 0
        and features % COLUMNS == 0
        and len(chunk_sizes(channels // GROUP, n_r)) > TAIL
        and all(divided(n_r, n_c, length_first, length_second, size) for size in chunk_sizes(channels // GROUP, n_r))
    )


def tables(length):
    series = jnp.arange(length, dtype=jnp.int32)
    product = series[:, None] * series[None, :] % length
    angles = product.astype(jnp.float32) * (2.0 * math.pi / length)
    return (jnp.cos(angles), jnp.sin(angles))


def folded_order(length_first, devices):
    block = length_first // devices
    half_block = block // 2
    series = jnp.arange(length_first, dtype=jnp.int32)
    device = series // block
    inner = series % block
    lower = device * half_block + inner
    upper = length_first - device * half_block - (inner - half_block)
    upper = jnp.where((device == 0) & (inner == half_block), length_first // 2, upper)
    return jnp.where(inner < half_block, lower, upper) % length_first


def to_channels(values, row_count):
    rows_first, rows_second, channels = values.shape
    width = channels // row_count
    parted = values.reshape(rows_first, rows_second, row_count, width).transpose(2, 0, 1, 3)
    return parted.reshape(row_count * rows_first, rows_second * width)


def product(table, values):
    return jnp.dot(table, values, precision=highest)


def middle(real_part, imag_part, width):
    length_first = real_part.shape[0]
    rows_second = real_part.shape[1] // width
    col_count = lax.axis_size("col")
    length_second = rows_second * col_count
    positions = length_first * length_second
    frequency = folded_order(length_first, col_count)
    series = jnp.arange(length_first, dtype=jnp.int32)
    first_angle = (frequency[:, None] * series[None, :] % length_first).astype(jnp.float32)
    first_angle = first_angle * (2.0 * math.pi / length_first)
    first_cos = jnp.cos(first_angle)
    first_sin = jnp.sin(first_angle)
    first_real = product(first_cos, real_part)
    first_imag = -product(first_sin, real_part)
    first_real = first_real + product(first_sin, imag_part)
    first_imag = first_imag + product(first_cos, imag_part)
    first_real = first_real.reshape(length_first, rows_second, width)
    first_imag = first_imag.reshape(length_first, rows_second, width)
    second_index = lax.axis_index("col") * rows_second + jnp.arange(rows_second, dtype=jnp.int32)
    twiddle_angle = (frequency[:, None] * second_index[None, :] % positions).astype(jnp.float32)
    twiddle_angle = twiddle_angle * (2.0 * math.pi / positions)
    twiddle_cos = jnp.cos(twiddle_angle)[:, :, None]
    twiddle_sin = jnp.sin(twiddle_angle)[:, :, None]
    turned_real = first_real * twiddle_cos + first_imag * twiddle_sin
    turned_imag = first_imag * twiddle_cos - first_real * twiddle_sin
    turned = jnp.stack([turned_real, turned_imag]).transpose(0, 2, 1, 3)
    turned = turned.reshape(2, rows_second, length_first * width)
    exchanged = lax.all_to_all(
        turned.astype(jnp.bfloat16), "col", split_axis=2, concat_axis=1, tiled=True
    ).astype(turned.dtype)
    second_cos, second_sin = tables(length_second)
    block = length_first // col_count
    out_shape = (length_second, block, width)
    out_real = (product(second_cos, exchanged[0]) + product(second_sin, exchanged[1])).reshape(
        out_shape
    )
    return out_real


def shards(tokens, norm_gain, w_in, w_out):
    rows_first, rows_second, features = tokens.shape
    row_count = lax.axis_size("row")
    length_first = rows_first * row_count
    length_second = rows_second * lax.axis_size("col")
    channels = w_in.shape[1]
    width = channels // row_count
    groups = channels // GROUP
    scaling = 1.0 / math.sqrt(length_first * length_second * GROUP)
    floats = tokens.astype(jnp.float32)
    normed = (
        floats
        * lax.rsqrt(jnp.mean(floats * floats, axis=-1, keepdims=True) + norm_eps)
        * norm_gain.astype(jnp.float32)
    ).astype(jnp.bfloat16)
    mapped = jnp.dot(normed.reshape(-1, features), w_in, preferred_element_type=jnp.float32)
    mapped = mapped.astype(jnp.bfloat16).reshape(rows_first, rows_second, channels)
    channel_cos, channel_sin = tables(GROUP)
    grouped = mapped.astype(jnp.float32).reshape(rows_first, rows_second, groups, GROUP)
    spec_real = jnp.einsum("abgj,jm->abgm", grouped, channel_cos, precision=highest)
    spec_imag = -jnp.einsum("abgj,jm->abgm", grouped, channel_sin, precision=highest)
    stacked = jnp.stack(
        [
            to_channels(spec_real.reshape(rows_first, rows_second, channels), row_count),
            to_channels(spec_imag.reshape(rows_first, rows_second, channels), row_count),
        ]
    )
    arrived = lax.all_to_all(
        stacked.astype(jnp.bfloat16), "row", split_axis=1, concat_axis=1, tiled=True
    ).astype(stacked.dtype)
    result = middle(arrived[0], arrived[1], width)
    spectrum = (result * scaling).astype(jnp.bfloat16)
    returned = lax.all_to_all(spectrum, "row", split_axis=0, concat_axis=2, tiled=True)
    mixed = jnp.dot(returned.reshape(-1, channels), w_out, preferred_element_type=jnp.float32)
    return mixed.astype(jnp.bfloat16).reshape(returned.shape[0], returned.shape[1], features)


def solution(mesh):
    in_specs = (P("row", "col", None), P(), P(), P())
    out_specs = P("row", "col", None)
    n_r, n_c = mesh.shape["row"], mesh.shape["col"]

    def run(tokens, norm_gain, w_in, w_out):
        whole = fits(n_r, n_c, tokens.shape, w_in.shape[1])
        body = functools.partial(fused_shards, n_r, n_c) if whole else shards
        return jax.shard_map(body, mesh=mesh, in_specs=in_specs, out_specs=out_specs, check_vma=False)(
            tokens, norm_gain, w_in, w_out
        )

    return run
```

```python
import functools
import math

import jax
import jax.numpy as jnp
import numpy as np
from jax import lax
from jax.experimental import pallas as pl
from jax.experimental.pallas import tpu as pltpu
from jax.sharding import PartitionSpec as P

GROUP = 128
LANES = 128
SUBLANES = 16
ROWS = 8
LAG = 4
TAIL = 2
HELD = 3
COLUMNS = 512
MESH = pl.DeviceIdType.MESH


norm_eps = 1e-06
highest = lax.Precision.HIGHEST


def folded_list(length_first, devices):
    block = length_first // devices
    half = block // 2
    result = np.zeros(length_first, np.int64)
    for device in range(devices):
        for inner in range(block):
            if inner < half:
                value = device * half + inner
            elif device == 0 and inner == half:
                value = length_first // 2
            else:
                value = length_first - device * half - (inner - half)
            result[device * block + inner] = value % length_first
    return result


def ceil_to(value, multiple):
    return -(-value // multiple) * multiple


class Piece:
    def __init__(self, groups, n_r, n_c, rows_first, rows_second, length_second):
        self.groups = groups
        self.channels = groups * GROUP
        self.used = groups * GROUP // n_r
        self.parts = LANES // self.used
        self.seconds = -(-rows_second // self.parts)
        self.block = rows_first * n_r // n_c
        self.rows1 = self.seconds * rows_first
        self.rows2 = ceil_to(self.seconds * self.block, ROWS)
        self.out_rows = length_second // n_r * self.block
        self.half = self.block // 2
        self.strips = self.parts // self.half
        self.step = self.out_rows // self.half // max(1, self.strips)
        self.rows3 = ceil_to(self.step, ROWS)
        depth = 2 * self.seconds
        ends = [(f * depth // ROWS * ROWS, ceil_to((f + 1) * depth, ROWS)) for f in range(self.half)]
        self.window = max(hi - lo for lo, hi in ends)
        self.lows = [min(lo, self.rows2 - self.window) for lo, _ in ends]


def chunk_sizes(groups, n_r):
    per = LANES // 2 // (GROUP // n_r)
    rest = groups % per
    return [per] * (groups // per) + ([rest] if rest else [])


def channel_tables(piece, n_r):
    width = GROUP // n_r
    half = width // 2
    j = np.arange(GROUP)
    forward = np.zeros((GROUP, n_r, width))
    back = np.zeros((n_r, piece.parts, piece.groups, width, piece.parts, piece.groups, GROUP))
    for row in range(n_r):
        for x in range(width):
            m = row * half + x % half
            cosine = x < half
            column = np.cos(2 * np.pi * j * m / GROUP) if cosine else np.sin(2 * np.pi * j * m / GROUP)
            entries = [(m, 1.0)]
            if not cosine and m == 0:
                column = np.cos(np.pi * j)
                entries = [(GROUP // 2, 1.0)]
            elif m:
                entries = [(m, 1.0 if cosine else -1.0), (GROUP - m, 1.0)]
            forward[:, row, x] = column
            for q in range(piece.parts):
                for g in range(piece.groups):
                    for at, sign in entries:
                        back[row, q, g, x, q, g, at] = sign
    size = piece.parts * piece.channels
    return forward.reshape(GROUP, LANES), back.reshape(n_r * LANES, size)


def position_tables(piece, rows_first, rows_second, n_r, n_c):
    length_first = rows_first * n_r
    length_second = rows_second * n_c
    positions = length_first * length_second
    block, parts, seconds = piece.block, piece.parts, piece.seconds
    half = block // 2
    a = np.arange(length_first)
    first = np.zeros((n_c, n_c, piece.rows2, n_r, seconds, rows_first))
    for col in range(n_c):
        for j in range(seconds):
            p = a * length_second + col * rows_second + j
            for target in range(n_c):
                for f_at in range(half):
                    f = target * half + f_at
                    angle = 2 * np.pi * (f * p % positions) / positions
                    real, imag = np.cos(angle), -np.sin(angle)
                    if f == 0:
                        real, imag = np.ones(length_first), (-1.0) ** a
                    first[col, target, 2 * (f_at * seconds + j), :, j, :] = real.reshape(n_r, rows_first)
                    first[col, target, 2 * (f_at * seconds + j) + 1, :, j, :] = imag.reshape(n_r, rows_first)
    k_b = np.arange(length_second)
    plain = np.zeros((2, 2, length_second, block, parts, n_c, piece.rows2))
    for other in range(2):
        for s in range(block):
            for source in range(n_c):
                for i in range(rows_second):
                    b = source * rows_second + i
                    f_at, upper = s % half, s >= half
                    q, j = divmod(i, seconds)
                    at = 2 * (f_at * seconds + j)
                    re_at, im_at = (q, source, at), (q, source, at + 1)
                    if other == 0 and f_at == 0:
                        shift = length_first // 2 if upper else 0
                        angle = 2 * np.pi * (b * (k_b * length_first + shift) % positions) / positions
                        place = im_at if upper else re_at
                        plain[(other, 0, slice(None), s) + place] = np.cos(angle)
                        plain[(other, 1, slice(None), s) + place] = np.sin(angle)
                        continue
                    sign = -1.0 if upper else 1.0
                    angle = 2 * np.pi * (b * (k_b + (1 if upper else 0)) % length_second) / length_second
                    plain[(other, 0, slice(None), s) + re_at] = np.cos(angle)
                    plain[(other, 0, slice(None), s) + im_at] = np.sin(angle) * sign
                    plain[(other, 1, slice(None), s) + re_at] = np.sin(angle)
                    plain[(other, 1, slice(None), s) + im_at] = -np.cos(angle) * sign
    plain = plain.reshape(2, 2, n_r, piece.out_rows, parts, n_c, piece.rows2) / math.sqrt(positions * GROUP)
    strips, step, window = piece.strips, piece.step, piece.window
    second = np.zeros((n_c, half, n_r, strips, 2, piece.rows3, parts, n_c, window))
    for col in range(n_c):
        mine = plain[min(col, 1)].copy()
        for f_at in range(half):
            f = col * half + f_at
            for q in range(parts if f else 0):
                turn = 2 * np.pi * (f * q * seconds % positions) / positions
                lo, hi = 2 * f_at * seconds, 2 * (f_at + 1) * seconds
                real, imag = mine[..., q, :, lo:hi:2].copy(), mine[..., q, :, lo + 1 : hi : 2].copy()
                mine[..., q, :, lo:hi:2] = real * np.cos(turn) - imag * np.sin(turn)
                mine[..., q, :, lo + 1 : hi : 2] = real * np.sin(turn) + imag * np.cos(turn)
        for f in range(half):
            low = piece.lows[f]
            for h in range(strips):
                rows = half * (h * step + np.arange(step)) + f
                for d in range(parts):
                    values = mine[:, :, rows, (f * strips + h - d) % parts, :, low : low + window]
                    second[col, f, :, h, :, :step, d] = values.transpose(1, 0, 2, 3, 4)
    first = first.reshape(n_c, n_c * piece.rows2, n_r * piece.rows1)
    return first, second.reshape(n_c, half, n_r * strips * 2 * piece.rows3, parts * n_c * window)


def bits_apart(one, other, count):
    total, bit = 0, 1
    while bit < count:
        total = total + bit * ((one // bit + other // bit) % 2)
        bit *= 2
    return total


def far_first(me, count):
    places = []
    for k in range(count - 1):
        down = count - 1 - k - jnp.where(count - 1 - k <= me, 1, 0)
        up = k + jnp.where(k >= me, 1, 0)
        places.append(jnp.where(me < count // 2, down, up))
    return places


def origin_first(me, count):
    places = far_first(me, count)
    inside = (me > 0) & (me < count // 2)
    return [jnp.where(inside, before, place) for before, place in zip([0] + places[:-1], places)]


def kernel(n_r, n_c, pieces, kinds, *refs):
    refs = list(refs)

    def take(count):
        taken = refs[:count]
        del refs[:count]
        return taken

    many = len(pieces)
    tokens, gain, w_in, w_out = take(4)
    (forward,) = take(1)
    tables_hbm = [take(3) for _ in pieces]
    partial, spectrum, tail_w = take(3)
    tok_v, gain_v, norm_v, win_v, early_v, wout_v, forward_v, woven_v = take(8)
    tables_v = [take(3) for _ in pieces]
    buffers = [take(6) for _ in pieces]
    load_sem, send_sem, recv_sem = take(3)
    row, col = lax.axis_index("row"), lax.axis_index("col")
    rows, features = tokens.shape
    steps = len(kinds)
    spans, seats = [], []
    lo = 0
    for at, kind in enumerate(kinds):
        spans.append((lo, lo + pieces[kind].channels))
        seats.append(kinds[:at].count(kind))
        lo = spans[-1][1]

    barrier = pltpu.get_barrier_semaphore()
    for d in range(1, n_r):
        pl.semaphore_signal(barrier, inc=1, device_id={"row": bits_apart(row, d, n_r)}, device_id_type=MESH)
    for d in range(1, n_c):
        pl.semaphore_signal(barrier, inc=1, device_id={"col": bits_apart(col, d, n_c)}, device_id_type=MESH)

    load_tok = pltpu.make_async_copy(tokens, tok_v, load_sem.at[0])
    load_forward = pltpu.make_async_copy(forward, forward_v, load_sem.at[2])
    load_gain = pltpu.make_async_copy(gain, gain_v, load_sem.at[1])
    load_win = [
        pltpu.make_async_copy(w_in.at[:, lo:hi], win_v.at[:, lo:hi], load_sem.at[3 + t])
        for t, (lo, hi) in enumerate(spans)
    ]
    load = []
    for p, (first, second, back) in enumerate(tables_hbm):
        sources = (first.at[col], second.at[col], back)
        load.append(
            [
                pltpu.make_async_copy(x, y, load_sem.at[2 * p + n if n < 2 else 4 + p])
                for n, (x, y) in enumerate(zip(sources, tables_v[p]))
            ]
        )
    head = spans[steps - TAIL][0]
    load_wout = [
        pltpu.make_async_copy(w_out.at[:head], wout_v, load_sem.at[6]),
        pltpu.make_async_copy(w_out.at[head:], tail_w, load_sem.at[7]),
    ]
    load_tok.start()
    load_gain.start()
    load_forward.start()
    load_win[0].start()
    pending = {(p, n) for p in range(many) for n in range(3)}

    def table(p, n):
        if (p, n) in pending:
            load[p][n].wait()
            pending.discard((p, n))
        return tables_v[p][n]

    load_tok.wait()
    load_gain.wait()
    gains = gain_v[...].astype(jnp.float32)
    squares = jnp.zeros((rows, LANES), jnp.float32)
    for at in range(features // LANES):
        lanes = slice(at * LANES, (at + 1) * LANES)
        floats = tok_v[:, lanes].astype(jnp.float32)
        squares = squares + floats * floats
        norm_v[:, lanes] = (floats * gains[at : at + 1, :]).astype(jnp.bfloat16)
    inverse = lax.rsqrt(jnp.sum(squares, axis=-1, keepdims=True) / features + norm_eps)

    row_targets = far_first(row, n_r)
    col_targets = [k + jnp.where(k >= col, 1, 0) for k in range(n_c - 1)]
    stages = ((row, row_targets, "row"), (col, col_targets, "col"), (row, origin_first(row, n_r), "row"))

    def exchange(stage, t, span=slice(None)):
        p, seat = kinds[t], seats[t]
        sent, came = buffers[p][2 * stage : 2 * stage + 2]
        me, targets, axis = stages[stage]
        for target in targets[span]:
            pltpu.make_async_remote_copy(
                src_ref=sent.at[seat, target],
                dst_ref=came.at[seat, me],
                send_sem=send_sem.at[stage, p],
                recv_sem=recv_sem.at[stage, t],
                device_id={axis: target},
                device_id_type=MESH,
            ).start()

    def keep(stage, t):
        p, seat = kinds[t], seats[t]
        sent, came = buffers[p][2 * stage : 2 * stage + 2]
        me = stages[stage][0]
        pltpu.make_async_copy(sent.at[seat, me], came.at[seat, me], recv_sem.at[stage, t]).start()

    def arrived(stage, t):
        came = buffers[kinds[t]][2 * stage + 1].at[seats[t]]
        pltpu.make_async_copy(came, came, recv_sem.at[stage, t]).wait()
        return came

    def all_sent():
        for stage, (_, targets, _) in enumerate(stages):
            for p in range(many):
                gone = buffers[p][2 * stage].at[:, 0 : len(targets)]
                pltpu.make_async_copy(gone, gone, send_sem.at[stage, p]).wait()

    lane = lax.broadcasted_iota(jnp.int32, (1, LANES), 1)
    turn = lane % (GROUP // n_r)
    cosine = (turn < GROUP // n_r // 2) | ((turn == GROUP // n_r // 2) & (row == 0))

    def start(t):
        p, seat = kinds[t], seats[t]
        piece = pieces[p]
        lo, hi = spans[t]
        load_win[t].wait()
        if t == 0:
            load_forward.wait()
            for other in load_win[1:]:
                other.start()
            for n in range(2):
                for other in sorted(range(many), key=kinds.index):
                    load[other][n].start()
        mapped = jnp.dot(norm_v[...], win_v[:, lo:hi], preferred_element_type=jnp.float32) * inverse
        short = piece.parts * piece.rows1 - rows
        if short:
            mapped = jnp.concatenate([mapped, jnp.zeros((short, hi - lo), jnp.float32)], axis=0)
        blocks = [
            mapped[q * piece.rows1 : (q + 1) * piece.rows1, g * GROUP : (g + 1) * GROUP]
            for q in range(piece.parts)
            for g in range(piece.groups)
        ]
        side = jnp.concatenate(blocks, axis=0).astype(jnp.bfloat16)
        turned = jnp.dot(side, forward_v[...], preferred_element_type=jnp.float32)
        sent = buffers[p][0]
        width = GROUP // n_r
        for r in range(n_r):
            total = None
            for k in range(len(blocks)):
                strip = turned[k * piece.rows1 : (k + 1) * piece.rows1]
                if k != r:
                    strip = pltpu.roll(strip, (k - r) * width % LANES, 1)
                total = strip if total is None else jnp.where(lane < k * width, total, strip)
            sent[seat, r] = total.astype(jnp.bfloat16)
        if t == 0:
            pl.semaphore_wait(barrier, n_r + n_c - 2)
        exchange(0, t)
        keep(0, t)

    def middle_first(t):
        p, seat = kinds[t], seats[t]
        piece = pieces[p]
        weights = table(p, 0)
        values = arrived(0, t)[...].reshape(n_r * piece.rows1, LANES)
        total = jnp.dot(weights[...], values, preferred_element_type=jnp.float32)
        buffers[p][2][seat] = total.astype(jnp.bfloat16).reshape(n_c, piece.rows2, LANES)
        exchange(1, t)
        keep(1, t)

    def middle_second(t):
        p, seat = kinds[t], seats[t]
        piece = pieces[p]
        weights = table(p, 1)
        values = arrived(1, t)
        sent = buffers[p][4]
        size = piece.rows3
        count = n_c * piece.window
        chosen = []
        for f, low in enumerate(piece.lows):
            floats = values[:, low : low + piece.window].reshape(count, LANES).astype(jnp.float32)
            rolled = [floats] + [pltpu.roll(floats, d * piece.used, 1) for d in range(1, piece.parts)]
            deep = jnp.concatenate([part.astype(jnp.bfloat16) for part in rolled], axis=0)
            both = jnp.dot(weights[f], deep, preferred_element_type=jnp.float32)
            blocks = [both[n * size : (n + 1) * size] for n in range(2 * n_r * piece.strips)]
            chosen.append([jnp.where(cosine, *blocks[n : n + 2]) for n in range(0, len(blocks), 2)])
        for r in range(n_r):
            total = None
            for q in range(piece.parts):
                f, h = divmod(q, piece.strips)
                part = chosen[f][r * piece.strips + h]
                total = part if total is None else jnp.where(lane < q * piece.used, total, part)
            sent[seat, r] = total.astype(jnp.bfloat16)
        exchange(2, t, slice(0, 1))
        if t < steps - HELD:
            exchange(2, t, slice(1, None))
        else:

            @pl.when(row < n_r // 2)
            def _():
                exchange(2, t, slice(1, None))

        if t == steps - 1:

            @pl.when(row >= n_r // 2)
            def _():
                for held in range(steps - HELD, steps):
                    exchange(2, held, slice(1, None))

        keep(2, t)

    def finish(t):
        p, seat = kinds[t], seats[t]
        piece = pieces[p]
        lo, hi = spans[t]
        weights = table(p, 2)
        came = arrived(2, t)
        side = jnp.concatenate([came[r] for r in range(n_r)], axis=1)
        total = jnp.dot(side, weights[...], preferred_element_type=jnp.float32)
        size, step = piece.channels, piece.step
        place, lo = (early_v, lo) if t < steps - TAIL else (spectrum, lo - head)
        for q in range(piece.parts):
            f, h = divmod(q, piece.strips)
            for c in range(size // LANES):
                at = q * size + c * LANES
                woven_v[c, pl.ds(piece.half * h * step + f, step, stride=piece.half), :] = total[:step, at : at + LANES]
        for c in range(size // LANES):
            place[:, lo + c * LANES : lo + (c + 1) * LANES] = woven_v[c].astype(jnp.bfloat16)
        if t == steps - TAIL - 1:
            load_wout[0].wait()
            for at in range(0, features, COLUMNS):
                columns = slice(at, at + COLUMNS)
                partial[:, columns] = jnp.dot(early_v[...], wout_v[:, columns], preferred_element_type=jnp.float32)
            load_wout[1].wait()

    for t in range(steps):
        start(t)
    for p in range(many):
        load[p][2].start()
    for copy in load_wout:
        copy.start()
    for job, t in schedule(steps):
        (middle_first, middle_second, finish)[job](t)
    all_sent()


def schedule(steps):
    jobs = [(0, t) for t in range(steps)]
    jobs[min(LAG, steps) : min(LAG, steps)] = [(1, 0)]
    return jobs + [(1, t) for t in range(1, steps)] + [(2, t) for t in range(steps)]


def last_product(partial, spectrum, w_tail, out, out_v, sems):
    copies = []
    for n, at in enumerate(range(0, partial.shape[1], COLUMNS)):
        columns = slice(at, at + COLUMNS)
        total = jnp.dot(spectrum[...], w_tail[:, columns], preferred_element_type=jnp.float32)
        total = total + partial[:, columns]
        out_v[:, :, columns] = total.reshape(*out_v.shape[:2], COLUMNS).astype(jnp.bfloat16)
        copy = pltpu.make_async_copy(out_v.at[:, :, columns], out.at[:, :, columns], sems.at[n])
        copy.start()
        copies.append(copy)
    for copy in copies:
        copy.wait()


def fused_shards(n_r, n_c, tokens, norm_gain, w_in, w_out):
    rows_first, rows_second, features = tokens.shape
    channels = w_in.shape[1]
    length_second = rows_second * n_c
    sizes = chunk_sizes(channels // GROUP, n_r)
    distinct = sorted(set(sizes))
    kinds = [distinct.index(size) for size in sizes]
    pieces = [Piece(size, n_r, n_c, rows_first, rows_second, length_second) for size in distinct]
    block, out_rows = pieces[0].block, pieces[0].out_rows
    head = sum(sizes[:-TAIL]) * GROUP
    rows = rows_first * rows_second
    tokens = tokens.transpose(1, 0, 2).reshape(rows, features)
    kind = jnp.bfloat16
    tables = [channel_tables(pieces[0], n_r)[0]]
    for piece in pieces:
        _, back = channel_tables(piece, n_r)
        first, second = position_tables(piece, rows_first, rows_second, n_r, n_c)
        tables += [first, second, back]
    tables = [jnp.asarray(np.asarray(x, np.float32).astype(kind)) for x in tables]
    hbm = pl.BlockSpec(memory_space=pltpu.HBM)
    vmem = pl.BlockSpec(memory_space=pltpu.VMEM)
    dma = pltpu.SemaphoreType.DMA
    scratch = [
        pltpu.VMEM((rows, features), kind),
        pltpu.VMEM((features // LANES, LANES), kind),
        pltpu.VMEM((rows, features), kind),
        pltpu.VMEM(w_in.shape, kind),
        pltpu.VMEM((out_rows, head), kind),
        pltpu.VMEM((head, features), kind),
        pltpu.VMEM(tables[0].shape, kind),
        pltpu.VMEM((max(sizes) * GROUP // LANES, out_rows, LANES), jnp.float32),
    ]
    for p in range(len(pieces)):
        first, second, back = tables[3 * p + 1 : 3 * p + 4]
        scratch += [pltpu.VMEM(x, kind) for x in (first.shape[1:], second.shape[1:], back.shape)]
    for p, piece in enumerate(pieces):
        count = kinds.count(p)
        for first_size, second_size in ((n_r, piece.rows1), (n_c, piece.rows2), (n_r, piece.rows3)):
            scratch += [pltpu.VMEM((count, first_size, second_size, LANES), kind)] * 2
    steps = len(kinds)
    scratch += [dma((max(8, 3 + steps),)), dma((3, len(pieces))), dma((3, steps))]
    operands = (tokens, norm_gain.reshape(-1, LANES), w_in, w_out, *tables)
    partial, spectrum, w_tail = pl.pallas_call(
        functools.partial(kernel, n_r, n_c, pieces, kinds),
        out_shape=[
            pltpu.VMEM((out_rows, features), jnp.float32),
            pltpu.VMEM((out_rows, channels - head), kind),
            pltpu.VMEM((channels - head, features), kind),
        ],
        in_specs=[hbm] * len(operands),
        out_specs=[vmem] * 3,
        scratch_shapes=scratch,
        compiler_params=pltpu.CompilerParams(
            collective_id=0, has_side_effects=True, vmem_limit_bytes=53 * 1024 * 1024
        ),
    )(*[pltpu.with_memory_space_constraint(x, pltpu.HBM) for x in operands])
    out_shape = (length_second // n_r, block, features)
    return pl.pallas_call(
        last_product,
        out_shape=jax.ShapeDtypeStruct(out_shape, kind),
        in_specs=[vmem] * 3,
        out_specs=hbm,
        scratch_shapes=[pltpu.VMEM(out_shape, kind), dma((features // COLUMNS,))],
        compiler_params=pltpu.CompilerParams(vmem_limit_bytes=16 * 1024 * 1024),
    )(partial, spectrum, w_tail)


def divided(n_r, n_c, length_first, length_second, size):
    used, half = size * GROUP // n_r, length_first // n_c // 2
    out_rows = length_second // n_r * 2 * half
    return LANES % (used * half) == 0 and out_rows % (LANES // used) == 0


def fits(n_r, n_c, tokens_shape, channels):
    length_first, length_second, features = tokens_shape
    return (
        n_r > 1
        and n_c & (n_c - 1) == 0
        and GROUP % (2 * n_r) == 0
        and length_first % (2 * n_c) == 0
        and SUBLANES % (length_first // n_c) == 0
        and length_first // n_r % ROWS == 0
        and length_second // n_r * (length_first // n_c) % ROWS == 0
        and length_second % n_r == 0
        and features % COLUMNS == 0
        and len(chunk_sizes(channels // GROUP, n_r)) > TAIL
        and all(divided(n_r, n_c, length_first, length_second, size) for size in chunk_sizes(channels // GROUP, n_r))
    )


def tables(length):
    series = jnp.arange(length, dtype=jnp.int32)
    product = series[:, None] * series[None, :] % length
    angles = product.astype(jnp.float32) * (2.0 * math.pi / length)
    return (jnp.cos(angles), jnp.sin(angles))


def folded_order(length_first, devices):
    block = length_first // devices
    half_block = block // 2
    series = jnp.arange(length_first, dtype=jnp.int32)
    device = series // block
    inner = series % block
    lower = device * half_block + inner
    upper = length_first - device * half_block - (inner - half_block)
    upper = jnp.where((device == 0) & (inner == half_block), length_first // 2, upper)
    return jnp.where(inner < half_block, lower, upper) % length_first


def to_channels(values, row_count):
    rows_first, rows_second, channels = values.shape
    width = channels // row_count
    parted = values.reshape(rows_first, rows_second, row_count, width).transpose(2, 0, 1, 3)
    return parted.reshape(row_count * rows_first, rows_second * width)


def product(table, values):
    return jnp.dot(table, values, precision=highest)


def middle(real_part, imag_part, width):
    length_first = real_part.shape[0]
    rows_second = real_part.shape[1] // width
    col_count = lax.axis_size("col")
    length_second = rows_second * col_count
    positions = length_first * length_second
    frequency = folded_order(length_first, col_count)
    series = jnp.arange(length_first, dtype=jnp.int32)
    first_angle = (frequency[:, None] * series[None, :] % length_first).astype(jnp.float32)
    first_angle = first_angle * (2.0 * math.pi / length_first)
    first_cos = jnp.cos(first_angle)
    first_sin = jnp.sin(first_angle)
    first_real = product(first_cos, real_part)
    first_imag = -product(first_sin, real_part)
    first_real = first_real + product(first_sin, imag_part)
    first_imag = first_imag + product(first_cos, imag_part)
    first_real = first_real.reshape(length_first, rows_second, width)
    first_imag = first_imag.reshape(length_first, rows_second, width)
    second_index = lax.axis_index("col") * rows_second + jnp.arange(rows_second, dtype=jnp.int32)
    twiddle_angle = (frequency[:, None] * second_index[None, :] % positions).astype(jnp.float32)
    twiddle_angle = twiddle_angle * (2.0 * math.pi / positions)
    twiddle_cos = jnp.cos(twiddle_angle)[:, :, None]
    twiddle_sin = jnp.sin(twiddle_angle)[:, :, None]
    turned_real = first_real * twiddle_cos + first_imag * twiddle_sin
    turned_imag = first_imag * twiddle_cos - first_real * twiddle_sin
    turned = jnp.stack([turned_real, turned_imag]).transpose(0, 2, 1, 3)
    turned = turned.reshape(2, rows_second, length_first * width)
    exchanged = lax.all_to_all(
        turned.astype(jnp.bfloat16), "col", split_axis=2, concat_axis=1, tiled=True
    ).astype(turned.dtype)
    second_cos, second_sin = tables(length_second)
    block = length_first // col_count
    out_shape = (length_second, block, width)
    out_real = (product(second_cos, exchanged[0]) + product(second_sin, exchanged[1])).reshape(
        out_shape
    )
    return out_real


def shards(tokens, norm_gain, w_in, w_out):
    rows_first, rows_second, features = tokens.shape
    row_count = lax.axis_size("row")
    length_first = rows_first * row_count
    length_second = rows_second * lax.axis_size("col")
    channels = w_in.shape[1]
    width = channels // row_count
    groups = channels // GROUP
    scaling = 1.0 / math.sqrt(length_first * length_second * GROUP)
    floats = tokens.astype(jnp.float32)
    normed = (
        floats
        * lax.rsqrt(jnp.mean(floats * floats, axis=-1, keepdims=True) + norm_eps)
        * norm_gain.astype(jnp.float32)
    ).astype(jnp.bfloat16)
    mapped = jnp.dot(normed.reshape(-1, features), w_in, preferred_element_type=jnp.float32)
    mapped = mapped.astype(jnp.bfloat16).reshape(rows_first, rows_second, channels)
    channel_cos, channel_sin = tables(GROUP)
    grouped = mapped.astype(jnp.float32).reshape(rows_first, rows_second, groups, GROUP)
    spec_real = jnp.einsum("abgj,jm->abgm", grouped, channel_cos, precision=highest)
    spec_imag = -jnp.einsum("abgj,jm->abgm", grouped, channel_sin, precision=highest)
    stacked = jnp.stack(
        [
            to_channels(spec_real.reshape(rows_first, rows_second, channels), row_count),
            to_channels(spec_imag.reshape(rows_first, rows_second, channels), row_count),
        ]
    )
    arrived = lax.all_to_all(
        stacked.astype(jnp.bfloat16), "row", split_axis=1, concat_axis=1, tiled=True
    ).astype(stacked.dtype)
    result = middle(arrived[0], arrived[1], width)
    spectrum = (result * scaling).astype(jnp.bfloat16)
    returned = lax.all_to_all(spectrum, "row", split_axis=0, concat_axis=2, tiled=True)
    mixed = jnp.dot(returned.reshape(-1, channels), w_out, preferred_element_type=jnp.float32)
    return mixed.astype(jnp.bfloat16).reshape(returned.shape[0], returned.shape[1], features)


def solution(mesh):
    in_specs = (P("row", "col", None), P(), P(), P())
    out_specs = P("row", "col", None)
    n_r, n_c = mesh.shape["row"], mesh.shape["col"]

    def run(tokens, norm_gain, w_in, w_out):
        whole = fits(n_r, n_c, tokens.shape, w_in.shape[1])
        body = functools.partial(fused_shards, n_r, n_c) if whole else shards
        return jax.shard_map(body, mesh=mesh, in_specs=in_specs, out_specs=out_specs, check_vma=False)(
            tokens, norm_gain, w_in, w_out
        )

    return run
```
